32 devices in a mesh: sp: 16 (over z, y, x), tp: 2 (over core).
Axes of the slice: x: 2, y: 2, z: 4, core: 2. Of those that a mesh axis runs over, the one named last changes fastest.
Arguments:
- prompt: bfloat16 [1, 8192, 2048], P(None, 'sp', 'tp'), may hold values from -6 to 6
- new_token: bfloat16 [1, 2048], P(None, 'tp'), may hold values from -6 to 6
- w_query: bfloat16 [2048, 2048], P(None, 'tp'), may hold values from -0.125 to 0.125
- w_key: bfloat16 [2048, 2048], P(None, 'tp'), may hold values from -0.125 to 0.125
- w_value: bfloat16 [2048, 2048], P(None, 'tp'), may hold values from -0.125 to 0.125
- decay_rate: float32 [16], P('tp'), may hold values from 1e-05 to 0.06
- norm_gain: float32 [2048], P('tp'), may hold values from 0.1 to 1.9
Outputs:
- mixed: bfloat16 [1, 8192, 2048], P(None, 'sp', 'tp')
- cache: bfloat16 [1, 16, 128, 128], P(None, 'tp', 'sp')
- new_read: bfloat16 [1, 2048], P(None, 'tp')
The draws below stay inside these ranges and needn't reach their ends.
All inputs are finite; a program needn't handle non-finite values.
Results may differ from the reference program's by a relative error of at most 0.0083.
Values may be sent and summed in bfloat16 or wider, within the bound.
A program may use at most 64 MiB of HBM per device.

```python
import jax
import jax.numpy as jnp
from jax import lax

D = 2048
H = 16
HEAD = 128
SEQS = 1
POS_DEV = 512
LEN = 8192


def draw_decay_rate(key, part):
    lowest = 1e-05
    highest = 0.06
    uniform_draw = jax.random.uniform(key, (H,), jnp.float32)
    return jnp.exp(jnp.log(lowest) + uniform_draw * (jnp.log(highest) - jnp.log(lowest)))


def shard_levels(rng, extent, pieces, smallest, high):
    def one(position, blocks):
        heights = jax.random.uniform(jax.random.fold_in(jax.random.fold_in(rng, 6), position), (blocks,), jnp.float32, smallest / len(pieces), high / len(pieces))
        return jnp.repeat(jnp.exp(heights), extent[position] // blocks).reshape((-1,) + (1,) * (len(extent) - position - 1))

    level = one(*pieces[0])
    for cut in pieces[1:]:
        level = level * one(*cut)
    return level


def gaussian(rng, shape, scale, reach, shards=(), held_as=jnp.bfloat16):
    result = jax.random.normal(rng, shape, jnp.float32) * scale
    if len(shards) > 0:
        result = shard_levels(rng, shape, shards, -0.22, 0.18) * result
    return jnp.clip(result, min=-reach, max=reach).astype(held_as)


def setup_inputs(seed: int = 0) -> dict:
    seeds = jax.random.split(jax.random.key(seed), 8)
    return {
        "prompt": gaussian(seeds[0], (SEQS, LEN, D), 1.0, 6.0, ((1, 16), (2, 2))),
        "new_token": gaussian(seeds[1], (SEQS, D), 1.0, 6.0, ((1, 2),)),
        "w_query": gaussian(seeds[2], (D, H * HEAD), D ** -0.5, 0.125, ((1, 2),)),
        "w_key": gaussian(seeds[3], (D, H * HEAD), D ** -0.5, 0.125, ((1, 2),)),
        "w_value": gaussian(seeds[4], (D, H * HEAD), D ** -0.5, 0.125, ((1, 2),)),
        "decay_rate": draw_decay_rate(jax.random.fold_in(seeds[7], 71), 0),
        "norm_gain": jnp.clip(1.0 + 0.18 * jax.random.normal(seeds[6], (H * HEAD,), jnp.float32), 0.1, 1.9),
    }


rope_base = 10000.0
norm_floor = 1e-05

def rotate(tensor, positions):
    head_width = tensor.shape[-1]
    inverse = rope_base ** (-jnp.arange(0, head_width, 2, dtype=jnp.float32) / head_width)
    angles = positions.astype(jnp.float32)[:, None] * inverse[None, :]
    cosine = jnp.cos(angles)[:, None, :]
    sine_part = jnp.sin(angles)[:, None, :]
    first_half = tensor[..., :head_width // 2]
    second_half = tensor[..., head_width // 2:]
    return jnp.concatenate([first_half * cosine - second_half * sine_part, first_half * sine_part + second_half * cosine], axis=-1)

def head_norm(output, gain):
    center = lax.optimization_barrier(jnp.mean(output, axis=-1, keepdims=True))
    spread = lax.optimization_barrier(jnp.mean(jnp.square(output - center), axis=-1, keepdims=True))
    return (output - center) * lax.rsqrt(spread + norm_floor) * gain

def decay_tables(log_gamma, block_size):
    offsets = jnp.arange(block_size, dtype=jnp.float32)
    gap_table = offsets[:, None] - offsets[None, :]
    within = jnp.where(gap_table[None] >= 0, jnp.exp(jnp.maximum(gap_table, 0.0)[None] * log_gamma[:, None, None]), 0.0)
    query_decay = jnp.exp((offsets[:, None] + 1.0) * log_gamma[None, :])
    key_decay = jnp.exp((block_size - 1.0 - offsets[:, None]) * log_gamma[None, :])
    return (within, query_decay, key_decay)

def project(token_rows, weight):
    return jnp.dot(token_rows, weight, preferred_element_type=jnp.float32).astype(jnp.bfloat16)

def reference(prompt, new_token, w_query, w_key, w_value, decay_rate, norm_gain):
    sequences, length, model_width = prompt.shape
    block_size = POS_DEV
    blocks = length // block_size
    token_rows = prompt.reshape(sequences * length, model_width)
    full_shape = (sequences, length, H, HEAD)
    queries = project(token_rows, w_query).reshape(full_shape)
    key_rows = project(token_rows, w_key).reshape(full_shape)
    values = project(token_rows, w_value).reshape(full_shape)
    positions = jnp.arange(length, dtype=jnp.int32)
    scaled = (rotate(queries.astype(jnp.float32), positions) * HEAD ** (-0.5)).astype(jnp.bfloat16)
    turned = rotate(key_rows.astype(jnp.float32), positions).astype(jnp.bfloat16)
    log_gamma = -decay_rate
    within, query_decay, key_decay = decay_tables(log_gamma, block_size)
    block_shape = (sequences, blocks, block_size, H, HEAD)

    def to_blocks(tensor):
        return jnp.moveaxis(tensor.reshape(block_shape), 1, 0)
    weighted = (to_blocks(turned).astype(jnp.float32) * key_decay[None, None, :, :, None]).astype(jnp.bfloat16)
    factor = jnp.exp(block_size * log_gamma)

    def advance(state_now, inputs):
        query_block, key_block, weighted_block, value_block = inputs
        scores = jnp.einsum('snhd,smhd->shnm', query_block.astype(jnp.float32), key_block.astype(jnp.float32)) * within[None]
        scores = lax.optimization_barrier(scores.astype(jnp.bfloat16)).astype(jnp.float32)
        inner_part = jnp.einsum('shnm,smhe->snhe', scores, value_block.astype(jnp.float32))
        state_read = lax.optimization_barrier(state_now.astype(jnp.bfloat16)).astype(jnp.float32)
        carried = jnp.einsum('snhd,shde->snhe', query_block.astype(jnp.float32), state_read) * query_decay[None, :, :, None]
        local_state = jnp.einsum('smhd,smhe->shde', weighted_block.astype(jnp.float32), value_block.astype(jnp.float32))
        return (state_now * factor[None, :, None, None] + local_state, inner_part + carried)
    initial = jnp.zeros((sequences, H, HEAD, HEAD), jnp.float32)
    final_state, outputs = lax.scan(advance, initial, (to_blocks(scaled), to_blocks(turned), weighted, to_blocks(values)))
    outputs = jnp.moveaxis(outputs, 0, 1).reshape(full_shape)
    gain = norm_gain.reshape(H, HEAD)
    mixed = head_norm(outputs, gain).astype(jnp.bfloat16).reshape(sequences, length, H * HEAD)
    cache = final_state.astype(jnp.bfloat16)
    token_shape = (sequences, 1, H, HEAD)
    token_query = project(new_token, w_query).reshape(token_shape)
    token_key = project(new_token, w_key).reshape(token_shape)
    token_value = project(new_token, w_value).reshape(token_shape)
    token_positions = jnp.full((1,), length, jnp.int32)
    token_scaled = (rotate(token_query.astype(jnp.float32), token_positions) * HEAD ** (-0.5)).astype(jnp.bfloat16)[:, 0]
    token_turned = rotate(token_key.astype(jnp.float32), token_positions).astype(jnp.bfloat16)[:, 0]
    from_cache = jnp.einsum('shd,shde->she', token_scaled.astype(jnp.float32), final_state, precision=lax.Precision.HIGHEST)
    own_score = lax.optimization_barrier(jnp.sum(token_scaled.astype(jnp.float32) * token_turned.astype(jnp.float32), axis=-1, keepdims=True))
    read_out = jnp.exp(log_gamma)[None, :, None] * from_cache + own_score * token_value[:, 0].astype(jnp.float32)
    new_read = head_norm(read_out, gain).astype(jnp.bfloat16).reshape(sequences, H * HEAD)
    return (mixed, cache, new_read)
```

```python
import functools

import jax
import jax.numpy as jnp
import numpy as np
from jax import lax
from jax.experimental import pallas as pl
from jax.experimental.pallas import tpu as pltpu
from jax.sharding import PartitionSpec as P

HEAD = 128
PAD = 16
rope_base = 10000.0
norm_floor = 1e-05
MESH = pl.DeviceIdType.MESH
BF = jnp.bfloat16
F32 = jnp.float32


def head_norm(o, gain):
    center = jnp.mean(o, axis=-1, keepdims=True)
    delta = o - center
    spread = jnp.mean(delta * delta, axis=-1, keepdims=True)
    return delta * lax.rsqrt(spread + norm_floor) * gain


def split(members):
    best = 1
    for g in range(1, members + 1):
        if members % g == 0 and g * g <= members:
            best = g
    return best


def dot(a, b):
    return jnp.dot(a, b, preferred_element_type=F32)


def kernel(cfg, x_hbm, tok_hbm, wq, wk, wv, rate_hbm, gain_hbm, tab_hbm, mixed, cache, read_out,
           rate, xbuf, wbuf, acc, tab, gain, ctab, stab, dec, kbuf, qbuf, vbuf, shi, slo, intra,
           send1, recv1, pre, tot, exc, upb, uprecv, down, downrecv, send3, recv3, tokq, tokk, tokv, rdbuf, tokbuf,
           w_sem, l_sem, tps, tpr, s1s, s1r, us, ur, ds, dr, s3s, s3r, rds, rdr, up_sem):
    M, G, Z, T, B, F, H, hc, R = cfg
    NC = H // hc
    W = hc * HEAD
    rank = lax.axis_index("sp")
    me = lax.axis_index("tp")
    z = rank // G
    j = rank % G
    weights = (wk, wv, wq)

    lx = pltpu.make_async_copy(x_hbm, xbuf.at[me, pl.ds(0, B)], l_sem.at[0])
    lr = pltpu.make_async_copy(rate_hbm, rate, l_sem.at[1])
    lt = pltpu.make_async_copy(tok_hbm, tokbuf, l_sem.at[2])
    ltab = pltpu.make_async_copy(tab_hbm, tab, l_sem.at[3])
    lg = pltpu.make_async_copy(gain_hbm, gain, l_sem.at[4])
    lx.start(priority=0)
    lr.start(priority=0)
    lt.start(priority=0)

    def wcopy(m, c, d, slot):
        p = lax.rem(me + d, T)
        return pltpu.make_async_copy(
            weights[m].at[pl.ds(pl.multiple_of(p * F, HEAD), F), pl.ds(c * W, W)],
            wbuf.at[m, c, d], w_sem.at[slot])

    def taken(ref, sem):
        pltpu.make_async_copy(ref, ref, sem).wait()

    for c in range(NC):
        wcopy(0, c, 0, c).start(priority=1)
        wcopy(1, c, 0, c).start(priority=1)

    barrier = pltpu.get_barrier_semaphore()
    for d in range(1, T):
        pl.semaphore_signal(barrier, inc=1, device_id={"tp": lax.rem(me + d, T)}, device_id_type=MESH)
    for d in range(1, G):
        pl.semaphore_signal(
            barrier, inc=1, device_id={"sp": z * G + lax.rem(j + d, G)}, device_id_type=MESH)
    for t in range(G, M):
        @pl.when(t // G > z)
        def _():
            pl.semaphore_signal(barrier, inc=1, device_id={"sp": t}, device_id_type=MESH)

    ltab.start(priority=1)
    for c in range(NC):
        for d in range(1, T):
            wcopy(0, c, d, NC).start(priority=1)
            wcopy(1, c, d, NC).start(priority=1)
    lg.start(priority=1)
    for c in range(NC):
        for d in range(T):
            wcopy(2, c, d, NC + 1).start(priority=1)

    lr.wait()
    ramp = (lax.broadcasted_iota(jnp.int32, (8, HEAD), 0) + 1).astype(F32)
    grow = [jnp.exp(ramp * rate[h]) for h in range(H)]
    leap = [jnp.exp(jnp.full((8, HEAD), 8.0 * rate[h], F32)) for h in range(H)]
    for n in range(0, B, 8):
        for h in range(H):
            dec[h, n:n + 8, :] = grow[h]
            grow[h] = grow[h] * leap[h]

    with jax.named_scope('w_x'):
        lx.wait()
    lt.wait()
    xbuf[me, B:B + PAD, :] = jnp.broadcast_to(tokbuf[...].astype(F32), (PAD, F)).astype(BF)

    def own_part(cs):
        for c in cs:
            taken(wbuf.at[pl.ds(0, 2), c, 0], w_sem.at[c])
        for c in cs:
            for m in range(2):
                acc[m, c] = dot(xbuf[me], wbuf[m, c, 0])

    with jax.named_scope('own0'):
        own_part([0])
    with jax.named_scope('w_bar'):
        pl.semaphore_wait(barrier, T - 1 + G - 1 + z * G)
    sends = []

    def xcopy(d, slot):
        return pltpu.make_async_remote_copy(
            src_ref=xbuf.at[slot], dst_ref=xbuf.at[slot], send_sem=tps.at[d - 1],
            recv_sem=tpr.at[d - 1], device_id={"tp": lax.rem(me + d, T)}, device_id_type=MESH)

    for d in range(1, T):
        cp = xcopy(d, me)
        cp.start()
        sends.append(cp)
    for t in range(M - G):
        @pl.when(t // G < z)
        def _():
            pl.semaphore_signal(up_sem, inc=1, device_id={"sp": t}, device_id_type=MESH)

    for cs in ([c] for c in range(1, NC)):
        with jax.named_scope(f'own{cs[0]}'):
            own_part(cs)

    ltab.wait()
    top = 2 * B
    spot = pl.multiple_of(top + rank * 16, 8)
    cb = tab[pl.ds(spot, 8), :][0:1]
    sb = tab[pl.ds(spot + 8, 8), :][0:1]
    ctab[0:B, :] = cb * tab[0:B, :] - sb * tab[B:top, :]
    stab[0:B, :] = sb * tab[0:B, :] + cb * tab[B:top, :]
    last = top + M * 16
    ctab[B:B + PAD, :] = jnp.broadcast_to(tab[last:last + 1, :], (PAD, HEAD))
    stab[B:B + PAD, :] = jnp.broadcast_to(tab[last + 8:last + 9, :], (PAD, HEAD))
    with jax.named_scope('w_wr'):
        if T > 1:
            taken(wbuf.at[pl.ds(0, 2), :, pl.ds(1, T - 1)], w_sem.at[NC])
    with jax.named_scope('w_tpx'):
        for d in range(1, T):
            xcopy(d, lax.rem(me + T - d, T)).wait_recv()

    def rotated(u):
        return u * ctab[...] + pltpu.roll(u, HEAD // 2, 1) * stab[...]

    def block_decay(c, power):
        rows = [jnp.exp(jnp.full((R, HEAD), -power * B * rate[c * hc + h], F32)) for h in range(hc)]
        return jnp.concatenate(rows, axis=0)

    def kv_dots(c):
        for m in range(2):
            total = acc[m, c]
            for d in range(1, T):
                total = total + dot(xbuf[lax.rem(me + d, T)], wbuf[m, c, d])
            acc[m, c] = total

    def kv_finish(c):
        states = []
        for hh in range(hc):
            h = c * hc + hh
            cols = slice(hh * HEAD, (hh + 1) * HEAD)
            kr = rotated(acc[0, c, :, cols])
            tokk[h:h + 1, :] = kr[B:B + 1]
            krb = kr[:B].astype(BF)
            kbuf[h] = krb
            v = acc[1, c, :, cols]
            tokv[h:h + 1, :] = v[B:B + 1]
            vb = (v[:B] * dec[h]).astype(BF)
            vbuf[h] = vb
            st = lax.dot_general(krb, vb, (((0,), (0,)), ((), ())), preferred_element_type=F32)
            st = st * jnp.exp(jnp.full((HEAD, HEAD), -B * rate[h], F32))
            hi = st.astype(BF)
            shi[h] = hi
            slo[h] = (st - hi.astype(F32)).astype(BF)
            states.append(st)
        for i in range(G):
            for zz in range(Z):
                lo = (zz * G + i) * R
                send1[c, i, zz] = jnp.concatenate([s[lo:lo + R] for s in states], axis=0).astype(BF)
        recv1[c, j] = send1[c, j]

    def kv_send(c):
        for d in range(1, G):
            i = lax.rem(j + d, G)
            cp = pltpu.make_async_remote_copy(
                src_ref=send1.at[c, i], dst_ref=recv1.at[c, j], send_sem=s1s.at[0],
                recv_sem=s1r.at[c], device_id={"sp": z * G + i}, device_id_type=MESH)
            cp.start()

    def plane_wait(c):
        taken(recv1.at[c, pl.ds(0, G - 1)], s1r.at[c])

    def faded(c, p):
        rows = [jnp.exp(jnp.full((R, HEAD), -G * B * rate[c * hc + h], F32) * p) for h in range(hc)]
        return jnp.concatenate(rows, axis=0)[None]

    levels = (Z - 1).bit_length()

    def up_send(c, level):
        if level >= levels:
            return

        @pl.when(z % (2 << level) == (1 << level) - 1)
        def _():
            upb[c] = (tot[c] + exc[c] * faded(c, 1.0)).astype(BF)
            for k in range(1, (1 << level) + 1):
                @pl.when(z + k < Z)
                def _():
                    pltpu.make_async_remote_copy(
                        src_ref=upb.at[c], dst_ref=uprecv.at[c, level], send_sem=us.at[0],
                        recv_sem=ur.at[c, level], device_id={"sp": (z + k) * G + j},
                        device_id_type=MESH).start()

    def plane(c):
        gb = block_decay(c, 1)[None]
        run = jnp.zeros((Z, hc * R, HEAD), F32)
        for i in range(G):
            pre[c, i] = run
            run = run * gb + recv1[c, i].astype(F32)
        tot[c] = run
        exc[c] = jnp.zeros((Z, hc * R, HEAD), F32)
        down[c] = run.astype(BF)
        for t in range(Z):
            @pl.when(t < z)
            def _():
                pltpu.make_async_remote_copy(
                    src_ref=down.at[c, t], dst_ref=downrecv.at[c, z], send_sem=ds.at[0],
                    recv_sem=dr.at[0], device_id={"sp": t * G + j}, device_id_type=MESH).start()
        up_send(c, 0)

    def climb(c, level):
        @pl.when((z // (1 << level)) % 2 == 1)
        def _():
            taken(uprecv.at[c, level], ur.at[c, level])
            p = (z % (1 << level)).astype(F32)
            exc[c] = exc[c] + uprecv[c, level].astype(F32) * faded(c, p)
        up_send(c, level + 1)

    def give_back(c):
        run = exc[c]
        gb = block_decay(c, 1)[None]
        for i in range(G):
            send3[c, i] = (run + pre[c, i]).astype(BF)
            run = run * gb
        recv3[c, j] = send3[c, j]
        for d in range(1, G):
            i = lax.rem(j + d, G)
            cp = pltpu.make_async_remote_copy(
                src_ref=send3.at[c, i], dst_ref=recv3.at[c, j], send_sem=s3s.at[0],
                recv_sem=s3r.at[c], device_id={"sp": z * G + i}, device_id_type=MESH)
            cp.start()

    def final():
        for k in range(1, Z):
            @pl.when(Z - 1 - z == k)
            def _():
                taken(downrecv.at[:, pl.ds(0, k)], dr.at[0])
        for c in range(NC):
            gz = faded(c, 1.0)[0]
            run = tot[c, z] + exc[c, z] * gz
            for s in range(1, Z):
                run = jnp.where(s > z, run * gz + downrecv[c, s].astype(F32), run)
            for hh in range(hc):
                cache[c * hc + hh] = run[hh * R:(hh + 1) * R].astype(BF)

    def q_project(cs):
        totals = []
        for c in cs:
            total = dot(xbuf[me], wbuf[2, c, 0])
            for d in range(1, T):
                total = total + dot(xbuf[lax.rem(me + d, T)], wbuf[2, c, d])
            totals.append(total)
        for c, total in zip(cs, totals):
            for hh in range(hc):
                h = c * hc + hh
                qr = rotated(total[:, hh * HEAD:(hh + 1) * HEAD])
                tokq[h:h + 1, :] = qr[B:B + 1]
                qbuf[h] = qr[:B].astype(BF)

    half = B // 2
    causal = (lax.broadcasted_iota(jnp.int32, (half, half), 0)
              >= lax.broadcasted_iota(jnp.int32, (half, half), 1))

    def attend(c):
        for hh in range(hc):
            h = c * hc + hh
            for t in range(2):
                rows = qbuf[h, t * half:(t + 1) * half, :]
                out = None
                for s in range(t + 1):
                    ks = kbuf[h, s * half:(s + 1) * half, :]
                    sc = lax.dot_general(rows, ks, (((1,), (1,)), ((), ())), preferred_element_type=F32)
                    if s == t:
                        sc = jnp.where(causal, sc, 0.0)
                    part = dot(sc.astype(BF), vbuf[h, s * half:(s + 1) * half, :])
                    out = part if out is None else out + part
                intra[h, t * half:(t + 1) * half, :] = out

    def tail_wait(c):
        taken(recv3.at[c, pl.ds(0, G - 1)], s3r.at[c])

    def tail(c):
        pieces = [[recv3[c, i, zz].astype(F32) for i in range(G)] for zz in range(Z)]
        for hh in range(hc):
            h = c * hc + hh
            inc = jnp.concatenate(
                [pieces[zz][i][hh * R:(hh + 1) * R] for zz in range(Z) for i in range(G)], axis=0)
            o = intra[h] + dot(qbuf[h], inc.astype(BF))
            delta = o - jnp.mean(o, axis=-1, keepdims=True)
            spread = jnp.mean(delta * delta, axis=-1, keepdims=True)
            up = dec[h]
            res = delta * lax.rsqrt(spread + (norm_floor * HEAD) * (up * up)) * gain[:, h * HEAD:(h + 1) * HEAD]
            mixed[:, h * HEAD:(h + 1) * HEAD] = res.astype(BF)

    def read_send():
        tq = jnp.concatenate([tokq[...], tokq[...]], axis=0).astype(BF)
        later = (M - 1 - rank).astype(F32)
        for h in range(H):
            got = dot(tq, shi[h]) + dot(tq, slo[h])
            fade = jnp.exp(jnp.full((1, HEAD), -B * rate[h], F32) * later)
            rdbuf[rank, h:h + 1, :] = got[h:h + 1] * fade
        for d in range(1, M):
            peer = lax.rem(rank + d, M)
            cp = pltpu.make_async_remote_copy(
                src_ref=rdbuf.at[rank], dst_ref=rdbuf.at[rank], send_sem=rds.at[0],
                recv_sem=rdr.at[0], device_id={"sp": peer}, device_id_type=MESH)
            cp.start()

    def read_finish():
        taken(rdbuf.at[pl.ds(0, M - 1)], rdr.at[0])
        total = jnp.sum(rdbuf[...], axis=0)
        scale = HEAD ** -0.5
        tq = tokq[...].astype(BF).astype(F32)
        tk = tokk[...].astype(BF).astype(F32)
        score = jnp.sum(tq * tk, axis=-1, keepdims=True) * scale
        base_part = score * tokv[...].astype(BF).astype(F32)
        for h in range(H):
            g = jnp.exp(jnp.full((1, HEAD), -rate[h], F32)) * scale
            o = g * total[h:h + 1] + base_part[h:h + 1]
            read_out[:, h * HEAD:(h + 1) * HEAD] = head_norm(o, gain[:, h * HEAD:(h + 1) * HEAD]).astype(BF)

    for c in range(NC):
        with jax.named_scope(f"kv{c}"):
            kv_dots(c)
            if c > 0:
                kv_finish(c - 1)
                kv_send(c - 1)
    with jax.named_scope("kvlast"):
        kv_finish(NC - 1)
        kv_send(NC - 1)
    with jax.named_scope("w_wq"):
        taken(wbuf.at[2], w_sem.at[NC + 1])
    groups = [range(c, min(c + 2, NC)) for c in range(0, NC, 2)]
    for n, cs in enumerate(groups):
        with jax.named_scope(f"q{n}"):
            q_project(cs)
    with jax.named_scope("w_up"):
        @pl.when(z < Z - 1)
        def _():
            pl.semaphore_wait(up_sem, (Z - 1 - z) * G)
    lg.wait()
    with jax.named_scope("rsend"):
        read_send()
    for c in range(NC):
        with jax.named_scope(f"w_plane{c}"):
            plane_wait(c)
        with jax.named_scope(f"plane{c}"):
            plane(c)
    todo = [[] for _ in range(NC)]
    for level in range(levels):
        for c in range(NC):
            todo[min(level, NC - 1)].append((c, level))
    for c in range(NC):
        with jax.named_scope(f"att{c}"):
            attend(c)
        for cc, level in todo[c]:
            with jax.named_scope(f"climb{cc}_{level}"):
                climb(cc, level)
                if level == levels - 1:
                    give_back(cc)
    with jax.named_scope("final"):
        final()
    for c in range(NC):
        with jax.named_scope(f"w_tail{c}"):
            tail_wait(c)
        with jax.named_scope(f"tail{c}"):
            tail(c)
    with jax.named_scope("rfin"):
        read_finish()
    with jax.named_scope("w_sends"):
        for cp in sends:
            cp.wait_send()
        taken(send1.at[:, pl.ds(0, G - 1)], s1s.at[0])
        taken(send3.at[:, pl.ds(0, G - 1)], s3s.at[0])
        taken(rdbuf.at[pl.ds(0, M - 1)], rds.at[0])
        for k in range(1, Z):
            @pl.when(z == k)
            def _():
                taken(down.at[:, pl.ds(0, k)], ds.at[0])
        for k in range(Z - 1):
            level = ((k + 1) & -(k + 1)).bit_length() - 1
            count = min(1 << level, Z - 1 - k)

            @pl.when(z == k)
            def _():
                taken(uprecv.at[:, pl.ds(0, 1)] if count == 1 else recv1.at[:, pl.ds(0, count)], us.at[0])


def flush(*refs):
    n = len(refs) // 2
    sems = refs[-1]
    copies = [pltpu.make_async_copy(refs[i], refs[n + i], sems.at[i]) for i in range(n)]
    for cp in copies:
        cp.start()
    for cp in copies:
        cp.wait()


def per_device(prompt, new_token, w_query, w_key, w_value, decay_rate, norm_gain):
    _, B, F = prompt.shape
    H = w_query.shape[1] // HEAD
    M = lax.axis_size("sp")
    T = lax.axis_size("tp")
    G = split(M)
    Z = M // G
    R = HEAD // M
    hc = 2 if H % 2 == 0 else 1
    NC = H // hc
    W = hc * HEAD
    inverse = rope_base ** (-np.arange(0, HEAD, 2, dtype=np.float64) / HEAD)
    sign = np.concatenate([-np.ones(HEAD // 2), np.ones(HEAD // 2)])

    def pair(positions):
        angles = np.concatenate([positions[:, None] * inverse[None]] * 2, axis=1)
        return np.cos(angles), np.sin(angles) * sign[None]

    tab = np.stack(pair(np.arange(B, dtype=np.float64))).astype(np.float32)
    base = np.stack(pair(np.arange(M + 1, dtype=np.float64) * B), axis=1).astype(np.float32)
    tab = np.concatenate([tab.reshape(2 * B, HEAD), np.repeat(base.reshape(2 * (M + 1), HEAD), 8, axis=0)])
    levels = (Z - 1).bit_length()
    any_ = pl.BlockSpec(memory_space=pltpu.HBM)
    vm = pl.BlockSpec(memory_space=pltpu.VMEM)
    V = pltpu.VMEM
    DMA = pltpu.SemaphoreType.DMA
    cfg = (M, G, Z, T, B, F, H, hc, R)
    shapes = ((B, H * HEAD), (H, R, HEAD), (1, H * HEAD))
    held = pl.pallas_call(
        functools.partial(kernel, cfg),
        out_shape=tuple(V(shape, BF) for shape in shapes),
        in_specs=[any_] * 8,
        out_specs=(vm, vm, vm),
        scratch_shapes=[
            pltpu.SMEM((H,), F32),
            V((T, B + PAD, F), BF),
            V((3, NC, T, F, W), BF),
            V((2, NC, B + PAD, W), F32),
            V(tab.shape, F32),
            V((1, H * HEAD), F32),
            V((B + PAD, HEAD), F32),
            V((B + PAD, HEAD), F32),
            V((H, B, HEAD), F32),
            V((H, B, HEAD), BF),
            V((H, B, HEAD), BF),
            V((H, B, HEAD), BF),
            V((H, HEAD, HEAD), BF),
            V((H, HEAD, HEAD), BF),
            V((H, B, HEAD), F32),
            V((NC, G, Z, hc * R, HEAD), BF),
            V((NC, G, Z, hc * R, HEAD), BF),
            V((NC, G, Z, hc * R, HEAD), F32),
            V((NC, Z, hc * R, HEAD), F32),
            V((NC, Z, hc * R, HEAD), F32),
            V((NC, Z, hc * R, HEAD), BF),
            V((NC, max(levels, 1), Z, hc * R, HEAD), BF),
            V((NC, Z, hc * R, HEAD), BF),
            V((NC, Z, hc * R, HEAD), BF),
            V((NC, G, Z, hc * R, HEAD), BF),
            V((NC, G, Z, hc * R, HEAD), BF),
            V((H, HEAD), F32),
            V((H, HEAD), F32),
            V((H, HEAD), F32),
            V((M, H, HEAD), F32),
            V((1, F), BF),
            DMA((NC + 2,)),
            DMA((5,)),
            DMA((max(T - 1, 1),)),
            DMA((max(T - 1, 1),)),
            DMA((1,)),
            DMA((NC,)),
            DMA((1,)),
            DMA((NC, max(levels, 1))),
            DMA((1,)),
            DMA((1,)),
            DMA((1,)),
            DMA((NC,)),
            DMA((1,)),
            DMA((1,)),
            pltpu.SemaphoreType.REGULAR,
        ],
        compiler_params=pltpu.CompilerParams(
            collective_id=0, has_side_effects=True, vmem_limit_bytes=60 * 1024 * 1024),
    )(prompt.reshape(B, F), new_token, w_query, w_key, w_value, decay_rate,
      norm_gain.reshape(1, H * HEAD), jnp.asarray(tab, F32))
    mixed, cache, new_read = pl.pallas_call(
        flush,
        out_shape=tuple(jax.ShapeDtypeStruct(shape, BF) for shape in shapes),
        in_specs=[vm] * len(shapes),
        out_specs=(any_,) * len(shapes),
        scratch_shapes=[DMA((len(shapes),))],
    )(*(pltpu.with_memory_space_constraint(a, V) for a in held))
    return (mixed[None], cache[None], new_read)


def solution(mesh):
    in_specs = (
        P(None, "sp", "tp"),
        P(None, "tp"),
        P(None, "tp"),
        P(None, "tp"),
        P(None, "tp"),
        P("tp"),
        P("tp"),
    )
    out_specs = (P(None, "sp", "tp"), P(None, "tp", "sp", None), P(None, "tp"))
    return jax.shard_map(
        per_device, mesh=mesh, in_specs=in_specs, out_specs=out_specs, check_vma=False
    )
```

```python
import functools

import jax
import jax.numpy as jnp
import numpy as np
from jax import lax
from jax.experimental import pallas as pl
from jax.experimental.pallas import tpu as pltpu
from jax.sharding import PartitionSpec as P

HEAD = 128
PAD = 16
rope_base = 10000.0
norm_floor = 1e-05
MESH = pl.DeviceIdType.MESH
BF = jnp.bfloat16
F32 = jnp.float32


def head_norm(o, gain):
    center = jnp.mean(o, axis=-1, keepdims=True)
    delta = o - center
    spread = jnp.mean(delta * delta, axis=-1, keepdims=True)
    return delta * lax.rsqrt(spread + norm_floor) * gain


def split(members):
    best = 1
    for g in range(1, members + 1):
        if members % g == 0 and g * g <= members:
            best = g
    return best


def dot(a, b):
    return jnp.dot(a, b, preferred_element_type=F32)


def kernel(cfg, x_hbm, tok_hbm, wq, wk, wv, rate_hbm, gain_hbm, tab_hbm, mixed, cache, read_out,
           rate, xbuf, wbuf, acc, tab, gain, ctab, stab, dec, floor, kbuf, qbuf, vbuf, early, shi, slo, intra,
           send1, recv1, pre, tot, exc, upb, uprecv, down, downrecv, send3, recv3, tokq, tokk, tokv, rd1, rd2, rd3, tokbuf,
           w_sem, l_sem, tps, tpr, s1s, s1r, us, ur, ds, dr, s3s, s3r, rds, rdr, up_sem):
    M, G, Z, T, B, F, H, hc, R = cfg
    NC = H // hc
    W = hc * HEAD
    rank = lax.axis_index("sp")
    me = lax.axis_index("tp")
    z = rank // G
    j = rank % G
    weights = (wk, wv, wq)

    lx = pltpu.make_async_copy(x_hbm, xbuf.at[me, pl.ds(0, B)], l_sem.at[0])
    lr = pltpu.make_async_copy(rate_hbm, rate, l_sem.at[1])
    lt = pltpu.make_async_copy(tok_hbm, tokbuf, l_sem.at[2])
    ltab = pltpu.make_async_copy(tab_hbm, tab, l_sem.at[3])
    lg = pltpu.make_async_copy(gain_hbm, gain, l_sem.at[4])
    lx.start(priority=0)
    lr.start(priority=0)
    lt.start(priority=0)

    def wcopy(m, c, d, slot):
        p = lax.rem(me + d, T)
        return pltpu.make_async_copy(
            weights[m].at[pl.ds(pl.multiple_of(p * F, HEAD), F), pl.ds(c * W, W)],
            wbuf.at[m, c, d], w_sem.at[slot])

    def taken(ref, sem):
        pltpu.make_async_copy(ref, ref, sem).wait()

    for c in range(NC):
        wcopy(0, c, 0, c).start(priority=1)
        wcopy(1, c, 0, c).start(priority=1)
    ltab.start(priority=1)

    barrier = pltpu.get_barrier_semaphore()
    for d in range(1, T):
        pl.semaphore_signal(barrier, inc=1, device_id={"tp": lax.rem(me + d, T)}, device_id_type=MESH)
    for d in range(1, G):
        pl.semaphore_signal(
            barrier, inc=1, device_id={"sp": z * G + lax.rem(j + d, G)}, device_id_type=MESH)
    for t in range(1, Z):
        @pl.when(t > z)
        def _():
            for i in range(G):
                pl.semaphore_signal(
                    barrier, inc=1, device_id={"sp": t * G + i}, device_id_type=MESH)

    for c in range(NC):
        for d in range(1, T):
            wcopy(0, c, d, NC).start(priority=1)
            wcopy(1, c, d, NC).start(priority=1)

    lr.wait()
    ramp = (lax.broadcasted_iota(jnp.int32, (8, HEAD), 0) + 1).astype(F32)
    grow = [jnp.exp(ramp * rate[h]) for h in range(H)]
    leap = [jnp.exp(jnp.full((8, HEAD), 8.0 * rate[h], F32)) for h in range(H)]
    for n in range(0, B, 8):
        for h in range(H):
            dec[h, n:n + 8, :] = grow[h]
            floor[h, n:n + 8, :] = grow[h] * grow[h] * (norm_floor * HEAD)
            grow[h] = grow[h] * leap[h]

    with jax.named_scope('w_x'):
        lx.wait()
    lt.wait()
    xbuf[me, B:B + PAD, :] = jnp.broadcast_to(tokbuf[...].astype(F32), (PAD, F)).astype(BF)

    def own_part(cs):
        for c in cs:
            taken(wbuf.at[pl.ds(0, 2), c, 0], w_sem.at[c])
        for c in cs:
            for m in range(2):
                acc[m, c] = dot(xbuf[me], wbuf[m, c, 0])

    with jax.named_scope('own0'):
        own_part([0])
    with jax.named_scope('w_bar'):
        pl.semaphore_wait(barrier, T - 1 + G - 1 + z * G)
    sends = []

    def xcopy(d, slot):
        return pltpu.make_async_remote_copy(
            src_ref=xbuf.at[slot], dst_ref=xbuf.at[slot], send_sem=tps.at[d - 1],
            recv_sem=tpr.at[d - 1], device_id={"tp": lax.rem(me + d, T)}, device_id_type=MESH)

    for d in range(1, T):
        cp = xcopy(d, me)
        cp.start()
        sends.append(cp)
    lg.start(priority=1)
    for c in range(NC):
        for d in range(T):
            wcopy(2, c, d, NC + 1).start(priority=1)
    for t in range(Z - 1):
        @pl.when(t < z)
        def _():
            pl.semaphore_signal(up_sem, inc=1, device_id={"sp": t * G + j}, device_id_type=MESH)

    for cs in ([c] for c in range(1, NC // 2)):
        own_part(cs)
    with jax.named_scope("own_last"):
        own_part(range(max(NC // 2, 1), NC))

    ltab.wait()
    top = 2 * B
    spot = pl.multiple_of(top + rank * 16, 8)
    cb = tab[pl.ds(spot, 8), :][0:1]
    sb = tab[pl.ds(spot + 8, 8), :][0:1]
    ctab[0:B, :] = cb * tab[0:B, :] - sb * tab[B:top, :]
    stab[0:B, :] = sb * tab[0:B, :] + cb * tab[B:top, :]
    last = top + M * 16
    ctab[B:B + PAD, :] = jnp.broadcast_to(tab[last:last + 1, :], (PAD, HEAD))
    stab[B:B + PAD, :] = jnp.broadcast_to(tab[last + 8:last + 9, :], (PAD, HEAD))
    with jax.named_scope('w_wr'):
        if T > 1:
            taken(wbuf.at[pl.ds(0, 2), :, pl.ds(1, T - 1)], w_sem.at[NC])
    with jax.named_scope('w_tpx'):
        for d in range(1, T):
            xcopy(d, lax.rem(me + T - d, T)).wait_recv()

    def rotated(u):
        return u * ctab[...] + pltpu.roll(u, HEAD // 2, 1) * stab[...]

    def block_decay(c, power):
        rows = [jnp.exp(jnp.full((R, HEAD), -power * B * rate[c * hc + h], F32)) for h in range(hc)]
        return jnp.concatenate(rows, axis=0)

    half = B // 2
    causal = (lax.broadcasted_iota(jnp.int32, (half, half), 0)
              >= lax.broadcasted_iota(jnp.int32, (half, half), 1))

    def kv_dots(c):
        for m in range(2):
            total = acc[m, c]
            for d in range(1, T):
                total = total + dot(xbuf[lax.rem(me + d, T)], wbuf[m, c, d])
            acc[m, c] = total

    def kv_finish(c):
        states = []
        for hh in range(hc):
            h = c * hc + hh
            cols = slice(hh * HEAD, (hh + 1) * HEAD)
            kr = rotated(acc[0, c, :, cols])
            tokk[h:h + 1, :] = kr[B:B + 1]
            krb = kr[:B].astype(BF)
            kbuf[h] = krb
            v = acc[1, c, :, cols]
            tokv[h:h + 1, :] = v[B:B + 1]
            vd = v[:B] * dec[h]
            vb = vd.astype(BF)
            vbuf[h] = (vd - jnp.mean(vd, axis=-1, keepdims=True)).astype(BF)
            first, second = (
                lax.dot_general(krb[lo:lo + half], vb[lo:lo + half], (((0,), (0,)), ((), ())), preferred_element_type=F32)
                for lo in (0, half))
            early[h] = first
            st = (first + second) * jnp.exp(jnp.full((HEAD, HEAD), -B * rate[h], F32))
            hi = st.astype(BF)
            shi[h] = hi
            slo[h] = (st - hi.astype(F32)).astype(BF)
            states.append(st)
        for i in range(G):
            for zz in range(Z):
                lo = (zz * G + i) * R
                send1[c, i, zz] = jnp.concatenate([s[lo:lo + R] for s in states], axis=0).astype(BF)
        recv1[c, j] = send1[c, j]

    def kv_send(c):
        for d in range(1, G):
            i = lax.rem(j + d, G)
            cp = pltpu.make_async_remote_copy(
                src_ref=send1.at[c, i], dst_ref=recv1.at[c, j], send_sem=s1s.at[0],
                recv_sem=s1r.at[c], device_id={"sp": z * G + i}, device_id_type=MESH)
            cp.start()

    def plane_wait(c):
        taken(recv1.at[c, pl.ds(0, G - 1)], s1r.at[c])

    def faded(c, p):
        rows = [jnp.exp(jnp.full((R, HEAD), -G * B * rate[c * hc + h], F32) * p) for h in range(hc)]
        return jnp.concatenate(rows, axis=0)[None]

    levels = (Z - 1).bit_length()

    def up_send(c, level):
        if level >= levels:
            return

        @pl.when(z % (2 << level) == (1 << level) - 1)
        def _():
            upb[c] = (tot[c] + exc[c] * faded(c, 1.0)).astype(BF)
            for k in range(1 << level, 0, -1):
                @pl.when(z + k < Z)
                def _():
                    pltpu.make_async_remote_copy(
                        src_ref=upb.at[c], dst_ref=uprecv.at[c, level], send_sem=us.at[0],
                        recv_sem=ur.at[c, level], device_id={"sp": (z + k) * G + j},
                        device_id_type=MESH).start()

    def plane(c):
        gb = block_decay(c, 1)[None]
        run = jnp.zeros((Z, hc * R, HEAD), F32)
        for i in range(G):
            pre[c, i] = run
            run = run * gb + recv1[c, i].astype(F32)
        tot[c] = run
        exc[c] = jnp.zeros((Z, hc * R, HEAD), F32)
        down[c] = run.astype(BF)
        for t in range(Z):
            @pl.when(t < z)
            def _():
                pltpu.make_async_remote_copy(
                    src_ref=down.at[c, t], dst_ref=downrecv.at[c, z], send_sem=ds.at[0],
                    recv_sem=dr.at[0], device_id={"sp": t * G + j}, device_id_type=MESH).start()
        up_send(c, 0)

        @pl.when(z == 0)
        def _():
            give_back(c)

    def climb(c, level):
        @pl.when((z // (1 << level)) % 2 == 1)
        def _():
            taken(uprecv.at[c, level], ur.at[c, level])
            p = (z % (1 << level)).astype(F32)
            exc[c] = exc[c] + uprecv[c, level].astype(F32) * faded(c, p)
        up_send(c, level + 1)

        @pl.when(z // (1 << level) == 1)
        def _():
            give_back(c)

    def give_back(c):
        run = exc[c]
        gb = block_decay(c, 1)[None]
        for i in range(G):
            send3[c, i] = (run + pre[c, i]).astype(BF)
            run = run * gb
        recv3[c, j] = send3[c, j]
        for d in range(1, G):
            i = lax.rem(j + d, G)
            cp = pltpu.make_async_remote_copy(
                src_ref=send3.at[c, i], dst_ref=recv3.at[c, j], send_sem=s3s.at[0],
                recv_sem=s3r.at[c], device_id={"sp": z * G + i}, device_id_type=MESH)
            cp.start()

    def final():
        for k in range(1, Z):
            @pl.when(Z - 1 - z == k)
            def _():
                taken(downrecv.at[:, pl.ds(0, k)], dr.at[0])
        for c in range(NC):
            gz = faded(c, 1.0)[0]
            run = tot[c, z] + exc[c, z] * gz
            for s in range(1, Z):
                run = jnp.where(s > z, run * gz + downrecv[c, s].astype(F32), run)
            for hh in range(hc):
                cache[c * hc + hh] = run[hh * R:(hh + 1) * R].astype(BF)

    def q_project(cs):
        totals = []
        for c in cs:
            total = dot(xbuf[me], wbuf[2, c, 0])
            for d in range(1, T):
                total = total + dot(xbuf[lax.rem(me + d, T)], wbuf[2, c, d])
            totals.append(total)
        for c, total in zip(cs, totals):
            for hh in range(hc):
                h = c * hc + hh
                qr = rotated(total[:, hh * HEAD:(hh + 1) * HEAD])
                tokq[h:h + 1, :] = qr[B:B + 1]
                qbuf[h] = qr[:B].astype(BF)

    def attend(c):
        for hh in range(hc):
            h = c * hc + hh
            for lo in (0, half):
                at = slice(lo, lo + half)
                sc = lax.dot_general(
                    qbuf[h, at, :], kbuf[h, at, :], (((1,), (1,)), ((), ())), preferred_element_type=F32)
                sc = jnp.where(causal, sc, 0.0).astype(BF)
                intra[h, at, :] = dot(sc, vbuf[h, at, :])

    def tail_wait(c):
        taken(recv3.at[c, pl.ds(0, G - 1)], s3r.at[c])

    def tail(c):
        pieces = [[recv3[c, i, zz].astype(F32) for i in range(G)] for zz in range(Z)]
        for hh in range(hc):
            h = c * hc + hh
            inc = jnp.concatenate(
                [pieces[zz][i][hh * R:(hh + 1) * R] for zz in range(Z) for i in range(G)], axis=0)
            for lo in (0, half):
                at = slice(lo, lo + half)
                held = inc if lo == 0 else inc + early[h]
                held = (held - jnp.mean(held, axis=-1, keepdims=True)).astype(BF)
                delta = intra[h, at, :] + dot(qbuf[h, at, :], held)
                spread = jnp.mean(delta * delta, axis=-1, keepdims=True)
                res = delta * lax.rsqrt(spread + floor[h, at, :]) * gain[:, h * HEAD:(h + 1) * HEAD]
                mixed[at, h * HEAD:(h + 1) * HEAD] = res.astype(BF)

    def read_send():
        tq = jnp.concatenate([tokq[...], tokq[...]], axis=0).astype(BF)
        later = (M - 1 - rank).astype(F32)
        for h in range(H):
            got = dot(tq, shi[h]) + dot(tq, slo[h])
            fade = jnp.exp(jnp.full((1, HEAD), -B * rate[h], F32) * later)
            rd1[j, h:h + 1, :] = got[h:h + 1] * fade
        for d in range(1, G):
            pltpu.make_async_remote_copy(
                src_ref=rd1.at[j], dst_ref=rd1.at[j], send_sem=rds.at[0], recv_sem=rdr.at[0],
                device_id={"sp": z * G + lax.rem(j + d, G)}, device_id_type=MESH).start()
        for t in range(Z - 1):
            @pl.when(t < z)
            def _():
                for i in range(G):
                    pltpu.make_async_remote_copy(
                        src_ref=rd1.at[j], dst_ref=rd3.at[rank], send_sem=rds.at[1], recv_sem=rdr.at[1],
                        device_id={"sp": t * G + i}, device_id_type=MESH).start()

    def read_relay():
        taken(rd1.at[pl.ds(0, G - 1)], rdr.at[0])
        rd2[z] = jnp.sum(rd1[...], axis=0)
        for t in range(1, Z):
            @pl.when(t > z)
            def _():
                pltpu.make_async_remote_copy(
                    src_ref=rd2.at[z], dst_ref=rd2.at[z], send_sem=rds.at[2], recv_sem=rdr.at[2],
                    device_id={"sp": t * G + j}, device_id_type=MESH).start()

    def read_finish():
        for k in range(1, Z):
            @pl.when(Z - 1 - z == k)
            def _():
                taken(rd3.at[pl.ds(0, k * G)], rdr.at[1])

            @pl.when(z == k)
            def _():
                taken(rd2.at[pl.ds(0, k)], rdr.at[2])
        total = rd2[z]
        for t in range(Z):
            if t < Z - 1:
                total = total + jnp.where(t < z, rd2[t], 0.0)
            if t > 0:
                total = total + jnp.where(t > z, jnp.sum(rd3[t * G:(t + 1) * G], axis=0), 0.0)
        scale = HEAD ** -0.5
        tq = tokq[...].astype(BF).astype(F32)
        tk = tokk[...].astype(BF).astype(F32)
        score = jnp.sum(tq * tk, axis=-1, keepdims=True) * scale
        base_part = score * tokv[...].astype(BF).astype(F32)
        for h in range(H):
            g = jnp.exp(jnp.full((1, HEAD), -rate[h], F32)) * scale
            o = g * total[h:h + 1] + base_part[h:h + 1]
            read_out[:, h * HEAD:(h + 1) * HEAD] = head_norm(o, gain[:, h * HEAD:(h + 1) * HEAD]).astype(BF)

    def before_q():
        with jax.named_scope("w_up"):
            @pl.when(z < Z - 1)
            def _():
                pl.semaphore_wait(up_sem, Z - 1 - z)
        lg.wait()
        with jax.named_scope("w_wq"):
            taken(wbuf.at[2], w_sem.at[NC + 1])

    def planes(cs):
        for c in cs:
            with jax.named_scope(f"w_plane{c}"):
                plane_wait(c)
            with jax.named_scope(f"plane{c}"):
                plane(c)

    def attends(cs):
        for c in cs:
            with jax.named_scope(f"att{c}"):
                attend(c)

    def climbs(cs, level):
        for c in cs:
            with jax.named_scope(f"climb{c}_{level}"):
                climb(c, level)

    for c in range(NC):
        if c == NC - 1:
            before_q()
        with jax.named_scope(f"kv{c}"):
            kv_dots(c)
            if c > 0:
                kv_finish(c - 1)
                kv_send(c - 1)
    with jax.named_scope("kvlast"):
        kv_finish(NC - 1)
        kv_send(NC - 1)
    groups = [range(c, min(c + 2, NC)) for c in range(0, NC, 2)]
    ready = 0
    for n, cs in enumerate(groups):
        with jax.named_scope(f"q{n}"):
            q_project(cs)
        if n < len(groups) - 1:
            for c in cs:
                attends([c])
                planes([ready])
                ready += 1
    planes(range(ready, NC))
    with jax.named_scope("rsend"):
        read_send()
    rest = list(groups[-1])
    step = 0
    if levels > 0:
        climbs([0], 0)
        step = 1
    for c in rest:
        attends([c])
        if levels > 0:
            more = NC if c == rest[-1] else min(step + 1, NC)
            climbs(range(step, more), 0)
            step = more
    for level in range(1, levels):
        climbs(range(NC), level)
    with jax.named_scope("w_relay"):
        read_relay()
    middle = Z // 2

    @pl.when(z >= middle)
    def _():
        with jax.named_scope("finala"):
            final()
    for n, cs in enumerate(groups):
        with jax.named_scope(f"w_tail{cs[0]}"):
            for c in cs:
                tail_wait(c)
        with jax.named_scope(f"tail{cs[0]}"):
            for c in cs:
                tail(c)
        if n == 0:
            @pl.when(z >= middle)
            def _():
                with jax.named_scope("w_rfina"):
                    read_finish()

    @pl.when(z < middle)
    def _():
        with jax.named_scope("final"):
            final()
        with jax.named_scope("w_rfin"):
            read_finish()
    with jax.named_scope("w_sends"):
        for cp in sends:
            cp.wait_send()
        taken(send1.at[:, pl.ds(0, G - 1)], s1s.at[0])
        taken(send3.at[:, pl.ds(0, G - 1)], s3s.at[0])
        taken(rd1.at[pl.ds(0, G - 1)], rds.at[0])
        for k in range(1, Z):
            @pl.when(z == k)
            def _():
                taken(down.at[:, pl.ds(0, k)], ds.at[0])
                taken(rd3.at[pl.ds(0, k * G)], rds.at[1])

            @pl.when(Z - 1 - z == k)
            def _():
                taken(rd2.at[pl.ds(0, k)], rds.at[2])
        for k in range(Z - 1):
            level = ((k + 1) & -(k + 1)).bit_length() - 1
            count = min(1 << level, Z - 1 - k)

            @pl.when(z == k)
            def _():
                taken(uprecv.at[:, pl.ds(0, 1)] if count == 1 else recv1.at[:, pl.ds(0, count)], us.at[0])


def flush(*refs):
    n = len(refs) // 2
    sems = refs[-1]
    copies = [pltpu.make_async_copy(refs[i], refs[n + i], sems.at[i]) for i in range(n)]
    for cp in copies:
        cp.start()
    for cp in copies:
        cp.wait()


def per_device(prompt, new_token, w_query, w_key, w_value, decay_rate, norm_gain):
    _, B, F = prompt.shape
    H = w_query.shape[1] // HEAD
    M = lax.axis_size("sp")
    T = lax.axis_size("tp")
    G = split(M)
    Z = M // G
    R = HEAD // M
    hc = 2 if H % 2 == 0 else 1
    NC = H // hc
    W = hc * HEAD
    inverse = rope_base ** (-np.arange(0, HEAD, 2, dtype=np.float64) / HEAD)
    sign = np.concatenate([-np.ones(HEAD // 2), np.ones(HEAD // 2)])

    def pair(positions):
        angles = np.concatenate([positions[:, None] * inverse[None]] * 2, axis=1)
        return np.cos(angles), np.sin(angles) * sign[None]

    tab = np.stack(pair(np.arange(B, dtype=np.float64))).astype(np.float32)
    base = np.stack(pair(np.arange(M + 1, dtype=np.float64) * B), axis=1).astype(np.float32)
    tab = np.concatenate([tab.reshape(2 * B, HEAD), np.repeat(base.reshape(2 * (M + 1), HEAD), 8, axis=0)])
    levels = (Z - 1).bit_length()
    any_ = pl.BlockSpec(memory_space=pltpu.HBM)
    vm = pl.BlockSpec(memory_space=pltpu.VMEM)
    V = pltpu.VMEM
    DMA = pltpu.SemaphoreType.DMA
    cfg = (M, G, Z, T, B, F, H, hc, R)
    shapes = ((B, H * HEAD), (H, R, HEAD), (1, H * HEAD))
    held = pl.pallas_call(
        functools.partial(kernel, cfg),
        out_shape=tuple(V(shape, BF) for shape in shapes),
        in_specs=[any_] * 8,
        out_specs=(vm, vm, vm),
        scratch_shapes=[
            pltpu.SMEM((H,), F32),
            V((T, B + PAD, F), BF),
            V((3, NC, T, F, W), BF),
            V((2, NC, B + PAD, W), F32),
            V(tab.shape, F32),
            V((1, H * HEAD), F32),
            V((B + PAD, HEAD), F32),
            V((B + PAD, HEAD), F32),
            V((H, B, HEAD), F32),
            V((H, B, HEAD), F32),
            V((H, B, HEAD), BF),
            V((H, B, HEAD), BF),
            V((H, B, HEAD), BF),
            V((H, HEAD, HEAD), F32),
            V((H, HEAD, HEAD), BF),
            V((H, HEAD, HEAD), BF),
            V((H, B, HEAD), F32),
            V((NC, G, Z, hc * R, HEAD), BF),
            V((NC, G, Z, hc * R, HEAD), BF),
            V((NC, G, Z, hc * R, HEAD), F32),
            V((NC, Z, hc * R, HEAD), F32),
            V((NC, Z, hc * R, HEAD), F32),
            V((NC, Z, hc * R, HEAD), BF),
            V((NC, max(levels, 1), Z, hc * R, HEAD), BF),
            V((NC, Z, hc * R, HEAD), BF),
            V((NC, Z, hc * R, HEAD), BF),
            V((NC, G, Z, hc * R, HEAD), BF),
            V((NC, G, Z, hc * R, HEAD), BF),
            V((H, HEAD), F32),
            V((H, HEAD), F32),
            V((H, HEAD), F32),
            V((G, H, HEAD), F32),
            V((Z, H, HEAD), F32),
            V((M, H, HEAD), F32),
            V((1, F), BF),
            DMA((NC + 2,)),
            DMA((5,)),
            DMA((max(T - 1, 1),)),
            DMA((max(T - 1, 1),)),
            DMA((1,)),
            DMA((NC,)),
            DMA((1,)),
            DMA((NC, max(levels, 1))),
            DMA((1,)),
            DMA((1,)),
            DMA((1,)),
            DMA((NC,)),
            DMA((3,)),
            DMA((3,)),
            pltpu.SemaphoreType.REGULAR,
        ],
        compiler_params=pltpu.CompilerParams(
            collective_id=0, has_side_effects=True, vmem_limit_bytes=60 * 1024 * 1024),
    )(prompt.reshape(B, F), new_token, w_query, w_key, w_value, decay_rate,
      norm_gain.reshape(1, H * HEAD), jnp.asarray(tab, F32))
    mixed, cache, new_read = pl.pallas_call(
        flush,
        out_shape=tuple(jax.ShapeDtypeStruct(shape, BF) for shape in shapes),
        in_specs=[vm] * len(shapes),
        out_specs=(any_,) * len(shapes),
        scratch_shapes=[DMA((len(shapes),))],
    )(*(pltpu.with_memory_space_constraint(a, V) for a in held))
    return (mixed[None], cache[None], new_read)


def solution(mesh):
    in_specs = (
        P(None, "sp", "tp"),
        P(None, "tp"),
        P(None, "tp"),
        P(None, "tp"),
        P(None, "tp"),
        P("tp"),
        P("tp"),
    )
    out_specs = (P(None, "sp", "tp"), P(None, "tp", "sp", None), P(None, "tp"))
    return jax.shard_map(
        per_device, mesh=mesh, in_specs=in_specs, out_specs=out_specs, check_vma=False
    )
```

```python
import functools

import jax
import jax.numpy as jnp
import numpy as np
from jax import lax
from jax.experimental import pallas as pl
from jax.experimental.pallas import tpu as pltpu
from jax.sharding import PartitionSpec as P

HEAD = 128
PAD = 16
rope_base = 10000.0
norm_floor = 1e-05
MESH = pl.DeviceIdType.MESH
BF = jnp.bfloat16
F32 = jnp.float32


def head_norm(o, gain):
    center = jnp.mean(o, axis=-1, keepdims=True)
    delta = o - center
    spread = jnp.mean(delta * delta, axis=-1, keepdims=True)
    return delta * lax.rsqrt(spread + norm_floor) * gain


def split(members):
    best = 1
    for g in range(1, members + 1):
        if members % g == 0 and g * g <= members:
            best = g
    return best


def dot(a, b):
    return jnp.dot(a, b, preferred_element_type=F32)


def kernel(cfg, x_hbm, tok_hbm, wq, wk, wv, rate_hbm, gain_hbm, tab_hbm, mixed, cache, read_out,
           rate, xbuf, wbuf, acc, tab, gain, ctab, stab, dec, floor, kbuf, qbuf, vbuf, early, shi, slo, intra,
           send1, recv1, pre, tot, exc, upb, uprecv, down, downrecv, send3, recv3, tokq, tokk, tokv, rd1, rd2, rd3, tokbuf,
           w_sem, l_sem, tps, tpr, s1s, s1r, us, ur, ds, dr, s3s, s3r, rds, rdr, up_sem):
    M, G, Z, T, B, F, H, hc, R = cfg
    NC = H // hc
    W = hc * HEAD
    rank = lax.axis_index("sp")
    me = lax.axis_index("tp")
    z = rank // G
    j = rank % G
    weights = (wk, wv, wq)

    lx = pltpu.make_async_copy(x_hbm, xbuf.at[me, pl.ds(0, B)], l_sem.at[0])
    lr = pltpu.make_async_copy(rate_hbm, rate, l_sem.at[1])
    lt = pltpu.make_async_copy(tok_hbm, tokbuf, l_sem.at[2])
    ltab = pltpu.make_async_copy(tab_hbm, tab, l_sem.at[3])
    lg = pltpu.make_async_copy(gain_hbm, gain, l_sem.at[4])
    lx.start(priority=0)
    lr.start(priority=0)
    lt.start(priority=0)

    def wcopy(m, c, d, slot):
        p = lax.rem(me + d, T)
        return pltpu.make_async_copy(
            weights[m].at[pl.ds(pl.multiple_of(p * F, HEAD), F), pl.ds(c * W, W)],
            wbuf.at[m, c, d], w_sem.at[slot])

    def taken(ref, sem):
        pltpu.make_async_copy(ref, ref, sem).wait()

    for c in range(NC):
        wcopy(0, c, 0, c).start(priority=1)
        wcopy(1, c, 0, c).start(priority=1)
    ltab.start(priority=1)

    barrier = pltpu.get_barrier_semaphore()
    for d in range(1, T):
        pl.semaphore_signal(barrier, inc=1, device_id={"tp": lax.rem(me + d, T)}, device_id_type=MESH)
    for d in range(1, G):
        pl.semaphore_signal(
            barrier, inc=1, device_id={"sp": z * G + lax.rem(j + d, G)}, device_id_type=MESH)
    for t in range(1, Z):
        @pl.when(t > z)
        def _():
            for i in range(G):
                pl.semaphore_signal(
                    barrier, inc=1, device_id={"sp": t * G + i}, device_id_type=MESH)

    for c in range(NC):
        for d in range(1, T):
            wcopy(0, c, d, NC).start(priority=1)
            wcopy(1, c, d, NC).start(priority=1)

    lr.wait()
    ramp = (lax.broadcasted_iota(jnp.int32, (8, HEAD), 0) + 1).astype(F32)
    grow = [jnp.exp(ramp * rate[h]) for h in range(H)]
    leap = [jnp.exp(jnp.full((8, HEAD), 8.0 * rate[h], F32)) for h in range(H)]
    for n in range(0, B, 8):
        for h in range(H):
            dec[h, n:n + 8, :] = grow[h]
            floor[h, n:n + 8, :] = grow[h] * grow[h] * (norm_floor * HEAD)
            grow[h] = grow[h] * leap[h]

    with jax.named_scope('w_x'):
        lx.wait()
    lt.wait()
    xbuf[me, B:B + PAD, :] = jnp.broadcast_to(tokbuf[...].astype(F32), (PAD, F)).astype(BF)

    def own_part(cs):
        for c in cs:
            taken(wbuf.at[pl.ds(0, 2), c, 0], w_sem.at[c])
        for c in cs:
            for m in range(2):
                acc[m, c] = dot(xbuf[me], wbuf[m, c, 0])

    with jax.named_scope('own0'):
        own_part([0])
    with jax.named_scope('w_bar'):
        pl.semaphore_wait(barrier, T - 1 + G - 1 + z * G)
    sends = []

    def xcopy(d, slot):
        return pltpu.make_async_remote_copy(
            src_ref=xbuf.at[slot], dst_ref=xbuf.at[slot], send_sem=tps.at[d - 1],
            recv_sem=tpr.at[d - 1], device_id={"tp": lax.rem(me + d, T)}, device_id_type=MESH)

    for d in range(1, T):
        cp = xcopy(d, me)
        cp.start()
        sends.append(cp)
    lg.start(priority=1)
    for c in range(NC):
        for d in range(T):
            wcopy(2, c, d, NC + 1).start(priority=1)
    for t in range(Z - 1):
        @pl.when(t < z)
        def _():
            pl.semaphore_signal(up_sem, inc=1, device_id={"sp": t * G + j}, device_id_type=MESH)

    for cs in ([c] for c in range(1, NC // 2)):
        own_part(cs)
    with jax.named_scope("own_last"):
        own_part(range(max(NC // 2, 1), NC))

    ltab.wait()
    top = 2 * B
    spot = pl.multiple_of(top + rank * 16, 8)
    cb = tab[pl.ds(spot, 8), :][0:1]
    sb = tab[pl.ds(spot + 8, 8), :][0:1]
    ctab[0:B, :] = cb * tab[0:B, :] - sb * tab[B:top, :]
    stab[0:B, :] = sb * tab[0:B, :] + cb * tab[B:top, :]
    last = top + M * 16
    ctab[B:B + PAD, :] = jnp.broadcast_to(tab[last:last + 1, :], (PAD, HEAD))
    stab[B:B + PAD, :] = jnp.broadcast_to(tab[last + 8:last + 9, :], (PAD, HEAD))
    with jax.named_scope('w_wr'):
        if T > 1:
            taken(wbuf.at[pl.ds(0, 2), :, pl.ds(1, T - 1)], w_sem.at[NC])
    with jax.named_scope('w_tpx'):
        for d in range(1, T):
            xcopy(d, lax.rem(me + T - d, T)).wait_recv()

    def rotated(u):
        return u * ctab[...] + pltpu.roll(u, HEAD // 2, 1) * stab[...]

    def block_decay(c, power):
        rows = [jnp.exp(jnp.full((R, HEAD), -power * B * rate[c * hc + h], F32)) for h in range(hc)]
        return jnp.concatenate(rows, axis=0)

    half = B // 2
    causal = (lax.broadcasted_iota(jnp.int32, (half, half), 0)
              >= lax.broadcasted_iota(jnp.int32, (half, half), 1))

    def kv_dots(c):
        for m in range(2):
            total = acc[m, c]
            for d in range(1, T):
                total = total + dot(xbuf[lax.rem(me + d, T)], wbuf[m, c, d])
            acc[m, c] = total

    def kv_finish(c):
        states = []
        for hh in range(hc):
            h = c * hc + hh
            cols = slice(hh * HEAD, (hh + 1) * HEAD)
            kr = rotated(acc[0, c, :, cols])
            tokk[h:h + 1, :] = kr[B:B + 1]
            krb = kr[:B].astype(BF)
            kbuf[h] = krb
            v = acc[1, c, :, cols]
            tokv[h:h + 1, :] = v[B:B + 1]
            vd = v[:B] * dec[h]
            vb = vd.astype(BF)
            vbuf[h] = (vd - jnp.mean(vd, axis=-1, keepdims=True)).astype(BF)
            first, second = (
                lax.dot_general(krb[lo:lo + half], vb[lo:lo + half], (((0,), (0,)), ((), ())), preferred_element_type=F32)
                for lo in (0, half))
            early[h] = first
            st = (first + second) * jnp.exp(jnp.full((HEAD, HEAD), -B * rate[h], F32))
            hi = st.astype(BF)
            shi[h] = hi
            slo[h] = (st - hi.astype(F32)).astype(BF)
            states.append(st)
        for i in range(G):
            for zz in range(Z):
                lo = (zz * G + i) * R
                send1[c, i, zz] = jnp.concatenate([s[lo:lo + R] for s in states], axis=0).astype(BF)
        recv1[c, j] = send1[c, j]

    def kv_send(c):
        for d in range(1, G):
            i = lax.rem(j + d, G)
            cp = pltpu.make_async_remote_copy(
                src_ref=send1.at[c, i], dst_ref=recv1.at[c, j], send_sem=s1s.at[0],
                recv_sem=s1r.at[c], device_id={"sp": z * G + i}, device_id_type=MESH)
            cp.start()

    def plane_wait(c):
        taken(recv1.at[c, pl.ds(0, G - 1)], s1r.at[c])

    def faded(c, p):
        rows = [jnp.exp(jnp.full((R, HEAD), -G * B * rate[c * hc + h], F32) * p) for h in range(hc)]
        return jnp.concatenate(rows, axis=0)[None]

    levels = (Z - 1).bit_length()

    def up_send(c, level):
        if level >= levels:
            return

        @pl.when(z % (2 << level) == (1 << level) - 1)
        def _():
            upb[c] = (tot[c] + exc[c] * faded(c, 1.0)).astype(BF)
            for k in range(1 << level, 0, -1):
                @pl.when(z + k < Z)
                def _():
                    pltpu.make_async_remote_copy(
                        src_ref=upb.at[c], dst_ref=uprecv.at[c, level], send_sem=us.at[0],
                        recv_sem=ur.at[c, level], device_id={"sp": (z + k) * G + j},
                        device_id_type=MESH).start()

    def plane(c):
        gb = block_decay(c, 1)[None]
        run = jnp.zeros((Z, hc * R, HEAD), F32)
        for i in range(G):
            pre[c, i] = run
            run = run * gb + recv1[c, i].astype(F32)
        tot[c] = run
        exc[c] = jnp.zeros((Z, hc * R, HEAD), F32)
        down[c] = run.astype(BF)
        for t in range(Z):
            @pl.when(t < z)
            def _():
                pltpu.make_async_remote_copy(
                    src_ref=down.at[c, t], dst_ref=downrecv.at[c, z], send_sem=ds.at[0],
                    recv_sem=dr.at[0], device_id={"sp": t * G + j}, device_id_type=MESH).start()
        up_send(c, 0)

        @pl.when(z == 0)
        def _():
            give_back(c)

    def climb(c, level):
        @pl.when((z // (1 << level)) % 2 == 1)
        def _():
            taken(uprecv.at[c, level], ur.at[c, level])
            p = (z % (1 << level)).astype(F32)
            exc[c] = exc[c] + uprecv[c, level].astype(F32) * faded(c, p)
        up_send(c, level + 1)

        @pl.when(z // (1 << level) == 1)
        def _():
            give_back(c)

    def give_back(c):
        run = exc[c]
        gb = block_decay(c, 1)[None]
        for i in range(G):
            send3[c, i] = (run + pre[c, i]).astype(BF)
            run = run * gb
        recv3[c, j] = send3[c, j]
        for d in range(1, G):
            i = lax.rem(j + d, G)
            cp = pltpu.make_async_remote_copy(
                src_ref=send3.at[c, i], dst_ref=recv3.at[c, j], send_sem=s3s.at[0],
                recv_sem=s3r.at[c], device_id={"sp": z * G + i}, device_id_type=MESH)
            cp.start()

    def final():
        for k in range(1, Z):
            @pl.when(Z - 1 - z == k)
            def _():
                taken(downrecv.at[:, pl.ds(0, k)], dr.at[0])
        for c in range(NC):
            gz = faded(c, 1.0)[0]
            run = tot[c, z] + exc[c, z] * gz
            for s in range(1, Z):
                run = jnp.where(s > z, run * gz + downrecv[c, s].astype(F32), run)
            for hh in range(hc):
                cache[c * hc + hh] = run[hh * R:(hh + 1) * R].astype(BF)

    def q_start(cs):
        row = (B + PAD) // 16 * 8
        for c in cs:
            for at in (slice(0, row), slice(row, B + PAD)):
                acc[0, c, at, :] = dot(xbuf[me, at, :], wbuf[2, c, 0])

    def q_project(cs, started):
        totals = []
        for c in cs:
            total = acc[0, c] if c in started else dot(xbuf[me], wbuf[2, c, 0])
            for d in range(1, T):
                total = total + dot(xbuf[lax.rem(me + d, T)], wbuf[2, c, d])
            totals.append(total)
        for c, total in zip(cs, totals):
            for hh in range(hc):
                h = c * hc + hh
                qr = rotated(total[:, hh * HEAD:(hh + 1) * HEAD])
                tokq[h:h + 1, :] = qr[B:B + 1]
                qbuf[h] = qr[:B].astype(BF)

    def attend(c):
        for hh in range(hc):
            h = c * hc + hh
            for lo in (0, half):
                at = slice(lo, lo + half)
                sc = lax.dot_general(
                    qbuf[h, at, :], kbuf[h, at, :], (((1,), (1,)), ((), ())), preferred_element_type=F32)
                sc = jnp.where(causal, sc, 0.0).astype(BF)
                intra[h, at, :] = dot(sc, vbuf[h, at, :])

    def tail_wait(c):
        taken(recv3.at[c, pl.ds(0, G - 1)], s3r.at[c])

    def tail(c):
        pieces = [[recv3[c, i, zz].astype(F32) for i in range(G)] for zz in range(Z)]
        for hh in range(hc):
            h = c * hc + hh
            inc = jnp.concatenate(
                [pieces[zz][i][hh * R:(hh + 1) * R] for zz in range(Z) for i in range(G)], axis=0)
            for lo in (0, half):
                at = slice(lo, lo + half)
                held = inc if lo == 0 else inc + early[h]
                held = (held - jnp.mean(held, axis=-1, keepdims=True)).astype(BF)
                delta = intra[h, at, :] + dot(qbuf[h, at, :], held)
                spread = jnp.mean(delta * delta, axis=-1, keepdims=True)
                res = delta * lax.rsqrt(spread + floor[h, at, :]) * gain[:, h * HEAD:(h + 1) * HEAD]
                mixed[at, h * HEAD:(h + 1) * HEAD] = res.astype(BF)

    def read_send():
        tq = jnp.concatenate([tokq[...], tokq[...]], axis=0).astype(BF)
        later = (M - 1 - rank).astype(F32)
        for h in range(H):
            got = dot(tq, shi[h]) + dot(tq, slo[h])
            fade = jnp.exp(jnp.full((1, HEAD), -B * rate[h], F32) * later)
            rd1[j, h:h + 1, :] = got[h:h + 1] * fade
        for d in range(1, G):
            pltpu.make_async_remote_copy(
                src_ref=rd1.at[j], dst_ref=rd1.at[j], send_sem=rds.at[0], recv_sem=rdr.at[0],
                device_id={"sp": z * G + lax.rem(j + d, G)}, device_id_type=MESH).start()
        for t in range(Z - 1):
            @pl.when(t < z)
            def _():
                for i in range(G):
                    pltpu.make_async_remote_copy(
                        src_ref=rd1.at[j], dst_ref=rd3.at[rank], send_sem=rds.at[1], recv_sem=rdr.at[1],
                        device_id={"sp": t * G + i}, device_id_type=MESH).start()

    def read_relay():
        taken(rd1.at[pl.ds(0, G - 1)], rdr.at[0])
        rd2[z] = jnp.sum(rd1[...], axis=0)
        for t in range(1, Z):
            @pl.when(t > z)
            def _():
                pltpu.make_async_remote_copy(
                    src_ref=rd2.at[z], dst_ref=rd2.at[z], send_sem=rds.at[2], recv_sem=rdr.at[2],
                    device_id={"sp": t * G + j}, device_id_type=MESH).start()

    def read_finish():
        for k in range(1, Z):
            @pl.when(Z - 1 - z == k)
            def _():
                taken(rd3.at[pl.ds(0, k * G)], rdr.at[1])

            @pl.when(z == k)
            def _():
                taken(rd2.at[pl.ds(0, k)], rdr.at[2])
        total = rd2[z]
        for t in range(Z):
            if t < Z - 1:
                total = total + jnp.where(t < z, rd2[t], 0.0)
            if t > 0:
                total = total + jnp.where(t > z, jnp.sum(rd3[t * G:(t + 1) * G], axis=0), 0.0)
        scale = HEAD ** -0.5
        tq = tokq[...].astype(BF).astype(F32)
        tk = tokk[...].astype(BF).astype(F32)
        score = jnp.sum(tq * tk, axis=-1, keepdims=True) * scale
        base_part = score * tokv[...].astype(BF).astype(F32)
        for h in range(H):
            g = jnp.exp(jnp.full((1, HEAD), -rate[h], F32)) * scale
            o = g * total[h:h + 1] + base_part[h:h + 1]
            read_out[:, h * HEAD:(h + 1) * HEAD] = head_norm(o, gain[:, h * HEAD:(h + 1) * HEAD]).astype(BF)

    def before_q():
        with jax.named_scope("w_up"):
            @pl.when(z < Z - 1)
            def _():
                pl.semaphore_wait(up_sem, Z - 1 - z)
        lg.wait()
        with jax.named_scope("w_wq"):
            taken(wbuf.at[2], w_sem.at[NC + 1])

    def planes(cs):
        for c in cs:
            with jax.named_scope(f"w_plane{c}"):
                plane_wait(c)
            with jax.named_scope(f"plane{c}"):
                plane(c)

    def attends(cs):
        for c in cs:
            with jax.named_scope(f"att{c}"):
                attend(c)

    def climbs(cs, level):
        for c in cs:
            with jax.named_scope(f"climb{c}_{level}"):
                climb(c, level)

    for c in range(NC):
        if c == NC - 1:
            before_q()
        with jax.named_scope(f"kv{c}"):
            kv_dots(c)
            if c > 0:
                kv_finish(c - 1)
                kv_send(c - 1)
    started = list(range(min(1, NC - 1)))
    with jax.named_scope("kvlast"):
        q_start(started)
        kv_finish(NC - 1)
        kv_send(NC - 1)
    groups = [range(c, min(c + 2, NC)) for c in range(0, NC, 2)]
    ready = 0
    for n, cs in enumerate(groups):
        with jax.named_scope(f"q{n}"):
            q_project(cs, started)
        if n < len(groups) - 1:
            for c in cs:
                attends([c])
                planes([ready])
                ready += 1
    planes(range(ready, NC))
    with jax.named_scope("rsend"):
        read_send()
    rest = list(groups[-1])
    step = 0
    if levels > 0:
        climbs(range(min(1, NC - 1)), 0)
        step = 1
    for c in rest:
        attends([c])
        if levels > 0:
            more = NC if c == rest[-1] else min(step + 1, NC)
            climbs(range(step, min(more, NC - 1)), 0)
            step = more
    if levels > 1:
        climbs([0], 1)
    if levels > 0:
        climbs([NC - 1], 0)
    for level in range(1, levels):
        climbs(range(1 if level == 1 else 0, NC), level)
    with jax.named_scope("w_relay"):
        read_relay()
    middle = Z // 2

    @pl.when(z >= middle)
    def _():
        with jax.named_scope("finala"):
            final()
    for n, cs in enumerate(groups):
        with jax.named_scope(f"w_tail{cs[0]}"):
            for c in cs:
                tail_wait(c)
        with jax.named_scope(f"tail{cs[0]}"):
            for c in cs:
                tail(c)
        if n == 0:
            @pl.when(z >= middle)
            def _():
                with jax.named_scope("w_rfina"):
                    read_finish()

    @pl.when(z < middle)
    def _():
        with jax.named_scope("final"):
            final()
        with jax.named_scope("w_rfin"):
            read_finish()
    with jax.named_scope("w_sends"):
        for cp in sends:
            cp.wait_send()
        taken(send1.at[:, pl.ds(0, G - 1)], s1s.at[0])
        taken(send3.at[:, pl.ds(0, G - 1)], s3s.at[0])
        taken(rd1.at[pl.ds(0, G - 1)], rds.at[0])
        for k in range(1, Z):
            @pl.when(z == k)
            def _():
                taken(down.at[:, pl.ds(0, k)], ds.at[0])
                taken(rd3.at[pl.ds(0, k * G)], rds.at[1])

            @pl.when(Z - 1 - z == k)
            def _():
                taken(rd2.at[pl.ds(0, k)], rds.at[2])
        for k in range(Z - 1):
            level = ((k + 1) & -(k + 1)).bit_length() - 1
            count = min(1 << level, Z - 1 - k)

            @pl.when(z == k)
            def _():
                taken(uprecv.at[:, pl.ds(0, 1)] if count == 1 else recv1.at[:, pl.ds(0, count)], us.at[0])


def flush(*refs):
    n = (len(refs) - 1) // 2
    sems = refs[-1]
    copies = []
    for i in range(n):
        rows = refs[i].shape[0]
        pieces = 4 if i == 0 else 1
        for k in range(pieces):
            at = pl.ds(k * (rows // pieces), rows // pieces)
            copies.append(pltpu.make_async_copy(refs[i].at[at], refs[n + i].at[at], sems.at[len(copies)]))
    for cp in copies:
        cp.start()
    for cp in copies:
        cp.wait()


def per_device(prompt, new_token, w_query, w_key, w_value, decay_rate, norm_gain):
    _, B, F = prompt.shape
    H = w_query.shape[1] // HEAD
    M = lax.axis_size("sp")
    T = lax.axis_size("tp")
    G = split(M)
    Z = M // G
    R = HEAD // M
    hc = 2 if H % 2 == 0 else 1
    NC = H // hc
    W = hc * HEAD
    inverse = rope_base ** (-np.arange(0, HEAD, 2, dtype=np.float64) / HEAD)
    sign = np.concatenate([-np.ones(HEAD // 2), np.ones(HEAD // 2)])

    def pair(positions):
        angles = np.concatenate([positions[:, None] * inverse[None]] * 2, axis=1)
        return np.cos(angles), np.sin(angles) * sign[None]

    tab = np.stack(pair(np.arange(B, dtype=np.float64))).astype(np.float32)
    base = np.stack(pair(np.arange(M + 1, dtype=np.float64) * B), axis=1).astype(np.float32)
    tab = np.concatenate([tab.reshape(2 * B, HEAD), np.repeat(base.reshape(2 * (M + 1), HEAD), 8, axis=0)])
    levels = (Z - 1).bit_length()
    any_ = pl.BlockSpec(memory_space=pltpu.HBM)
    vm = pl.BlockSpec(memory_space=pltpu.VMEM)
    V = pltpu.VMEM
    DMA = pltpu.SemaphoreType.DMA
    cfg = (M, G, Z, T, B, F, H, hc, R)
    shapes = ((B, H * HEAD), (H, R, HEAD), (1, H * HEAD))
    held = pl.pallas_call(
        functools.partial(kernel, cfg),
        out_shape=tuple(V(shape, BF) for shape in shapes),
        in_specs=[any_] * 8,
        out_specs=(vm, vm, vm),
        scratch_shapes=[
            pltpu.SMEM((H,), F32),
            V((T, B + PAD, F), BF),
            V((3, NC, T, F, W), BF),
            V((2, NC, B + PAD, W), F32),
            V(tab.shape, F32),
            V((1, H * HEAD), F32),
            V((B + PAD, HEAD), F32),
            V((B + PAD, HEAD), F32),
            V((H, B, HEAD), F32),
            V((H, B, HEAD), F32),
            V((H, B, HEAD), BF),
            V((H, B, HEAD), BF),
            V((H, B, HEAD), BF),
            V((H, HEAD, HEAD), F32),
            V((H, HEAD, HEAD), BF),
            V((H, HEAD, HEAD), BF),
            V((H, B, HEAD), F32),
            V((NC, G, Z, hc * R, HEAD), BF),
            V((NC, G, Z, hc * R, HEAD), BF),
            V((NC, G, Z, hc * R, HEAD), F32),
            V((NC, Z, hc * R, HEAD), F32),
            V((NC, Z, hc * R, HEAD), F32),
            V((NC, Z, hc * R, HEAD), BF),
            V((NC, max(levels, 1), Z, hc * R, HEAD), BF),
            V((NC, Z, hc * R, HEAD), BF),
            V((NC, Z, hc * R, HEAD), BF),
            V((NC, G, Z, hc * R, HEAD), BF),
            V((NC, G, Z, hc * R, HEAD), BF),
            V((H, HEAD), F32),
            V((H, HEAD), F32),
            V((H, HEAD), F32),
            V((G, H, HEAD), F32),
            V((Z, H, HEAD), F32),
            V((M, H, HEAD), F32),
            V((1, F), BF),
            DMA((NC + 2,)),
            DMA((5,)),
            DMA((max(T - 1, 1),)),
            DMA((max(T - 1, 1),)),
            DMA((1,)),
            DMA((NC,)),
            DMA((1,)),
            DMA((NC, max(levels, 1))),
            DMA((1,)),
            DMA((1,)),
            DMA((1,)),
            DMA((NC,)),
            DMA((3,)),
            DMA((3,)),
            pltpu.SemaphoreType.REGULAR,
        ],
        compiler_params=pltpu.CompilerParams(
            collective_id=0, has_side_effects=True, vmem_limit_bytes=60 * 1024 * 1024),
    )(prompt.reshape(B, F), new_token, w_query, w_key, w_value, decay_rate,
      norm_gain.reshape(1, H * HEAD), jnp.asarray(tab, F32))
    mixed, cache, new_read = pl.pallas_call(
        flush,
        out_shape=tuple(jax.ShapeDtypeStruct(shape, BF) for shape in shapes),
        in_specs=[vm] * len(shapes),
        out_specs=(any_,) * len(shapes),
        scratch_shapes=[DMA((len(shapes) + 3,))],
    )(*(pltpu.with_memory_space_constraint(a, V) for a in held))
    return (mixed[None], cache[None], new_read)


def solution(mesh):
    in_specs = (
        P(None, "sp", "tp"),
        P(None, "tp"),
        P(None, "tp"),
        P(None, "tp"),
        P(None, "tp"),
        P("tp"),
        P("tp"),
    )
    out_specs = (P(None, "sp", "tp"), P(None, "tp", "sp", None), P(None, "tp"))
    return jax.shard_map(
        per_device, mesh=mesh, in_specs=in_specs, out_specs=out_specs, check_vma=False
    )
```

```python
import functools

import jax
import jax.numpy as jnp
import numpy as np
from jax import lax
from jax.experimental import pallas as pl
from jax.experimental.pallas import tpu as pltpu
from jax.sharding import PartitionSpec as P

HEAD = 128
PAD = 16
rope_base = 10000.0
norm_floor = 1e-05
MESH = pl.DeviceIdType.MESH
BF = jnp.bfloat16
F32 = jnp.float32


def head_norm(o, gain):
    center = jnp.mean(o, axis=-1, keepdims=True)
    delta = o - center
    spread = jnp.mean(delta * delta, axis=-1, keepdims=True)
    return delta * lax.rsqrt(spread + norm_floor) * gain


def split(members):
    best = 1
    for g in range(1, members + 1):
        if members % g == 0 and g * g <= members:
            best = g
    return best


def dot(a, b):
    return jnp.dot(a, b, preferred_element_type=F32)


def kernel(cfg, x_hbm, tok_hbm, wq, wk, wv, rate_hbm, gain_hbm, tab_hbm, mixed, cache, read_out,
           rate, xbuf, wbuf, acc, tab, gain, ctab, stab, dec, floor, kbuf, qbuf, vbuf, early, shi, slo, intra,
           send1, recv1, pre, tot, exc, upb, uprecv, down, downrecv, send3, recv3, tokq, tokk, tokv, rd1, rd2, rd3, tokbuf,
           w_sem, l_sem, tps, tpr, s1s, s1r, us, ur, ds, dr, s3s, s3r, rds, rdr, up_sem):
    M, G, Z, T, B, F, H, hc, R = cfg
    NC = H // hc
    W = hc * HEAD
    rank = lax.axis_index("sp")
    me = lax.axis_index("tp")
    z = rank // G
    j = rank % G
    weights = (wk, wv, wq)

    lx = pltpu.make_async_copy(x_hbm, xbuf.at[me, pl.ds(0, B)], l_sem.at[0])
    lr = pltpu.make_async_copy(rate_hbm, rate, l_sem.at[1])
    lt = pltpu.make_async_copy(tok_hbm, tokbuf, l_sem.at[2])
    ltab = pltpu.make_async_copy(tab_hbm, tab, l_sem.at[3])
    lg = pltpu.make_async_copy(gain_hbm, gain, l_sem.at[4])
    lx.start(priority=0)
    lr.start(priority=0)
    lt.start(priority=0)

    def wcopy(m, c, d, slot):
        p = lax.rem(me + d, T)
        return pltpu.make_async_copy(
            weights[m].at[pl.ds(pl.multiple_of(p * F, HEAD), F), pl.ds(c * W, W)],
            wbuf.at[m, c, d], w_sem.at[slot])

    def taken(ref, sem):
        pltpu.make_async_copy(ref, ref, sem).wait()

    for c in range(NC):
        wcopy(0, c, 0, c).start(priority=1)
        wcopy(1, c, 0, c).start(priority=1)
    ltab.start(priority=1)

    barrier = pltpu.get_barrier_semaphore()
    for d in range(1, T):
        pl.semaphore_signal(barrier, inc=1, device_id={"tp": lax.rem(me + d, T)}, device_id_type=MESH)
    for d in range(1, G):
        pl.semaphore_signal(
            barrier, inc=1, device_id={"sp": z * G + lax.rem(j + d, G)}, device_id_type=MESH)
    for t in range(1, Z):
        @pl.when(t > z)
        def _():
            for i in range(G):
                pl.semaphore_signal(
                    barrier, inc=1, device_id={"sp": t * G + i}, device_id_type=MESH)

    for c in range(NC):
        for d in range(1, T):
            wcopy(0, c, d, NC).start(priority=1)
            wcopy(1, c, d, NC).start(priority=1)

    lr.wait()
    ramp = (lax.broadcasted_iota(jnp.int32, (8, HEAD), 0) + 1).astype(F32)
    grow = [jnp.exp(ramp * rate[h]) for h in range(H)]
    leap = [jnp.exp(jnp.full((8, HEAD), 8.0 * rate[h], F32)) for h in range(H)]
    for n in range(0, B, 8):
        for h in range(H):
            dec[h, n:n + 8, :] = grow[h]
            floor[h, n:n + 8, :] = grow[h] * grow[h] * (norm_floor * HEAD)
            grow[h] = grow[h] * leap[h]

    with jax.named_scope('w_x'):
        lx.wait()
    lt.wait()
    xbuf[me, B:B + PAD, :] = jnp.broadcast_to(tokbuf[...].astype(F32), (PAD, F)).astype(BF)

    def own_part(cs):
        for c in cs:
            taken(wbuf.at[pl.ds(0, 2), c, 0], w_sem.at[c])
        for c in cs:
            for m in range(2):
                acc[m, c] = dot(xbuf[me], wbuf[m, c, 0])

    with jax.named_scope('own0'):
        own_part([0])
    with jax.named_scope('w_bar'):
        pl.semaphore_wait(barrier, T - 1 + G - 1 + z * G)
    sends = []

    def xcopy(d, slot):
        return pltpu.make_async_remote_copy(
            src_ref=xbuf.at[slot], dst_ref=xbuf.at[slot], send_sem=tps.at[d - 1],
            recv_sem=tpr.at[d - 1], device_id={"tp": lax.rem(me + d, T)}, device_id_type=MESH)

    for d in range(1, T):
        cp = xcopy(d, me)
        cp.start()
        sends.append(cp)
    lg.start(priority=1)
    for c in range(NC):
        for d in range(T):
            wcopy(2, c, d, NC + 1).start(priority=1)
    for t in range(Z - 1):
        @pl.when(t < z)
        def _():
            pl.semaphore_signal(up_sem, inc=1, device_id={"sp": t * G + j}, device_id_type=MESH)

    with jax.named_scope("own_last"):
        own_part(range(1, NC))

    ltab.wait()
    top = 2 * B
    spot = pl.multiple_of(top + rank * 16, 8)
    cb = tab[pl.ds(spot, 8), :][0:1]
    sb = tab[pl.ds(spot + 8, 8), :][0:1]
    ctab[0:B, :] = cb * tab[0:B, :] - sb * tab[B:top, :]
    stab[0:B, :] = sb * tab[0:B, :] + cb * tab[B:top, :]
    last = top + M * 16
    ctab[B:B + PAD, :] = jnp.broadcast_to(tab[last:last + 1, :], (PAD, HEAD))
    stab[B:B + PAD, :] = jnp.broadcast_to(tab[last + 8:last + 9, :], (PAD, HEAD))
    with jax.named_scope('w_wr'):
        if T > 1:
            taken(wbuf.at[pl.ds(0, 2), :, pl.ds(1, T - 1)], w_sem.at[NC])
    with jax.named_scope('w_tpx'):
        for d in range(1, T):
            xcopy(d, lax.rem(me + T - d, T)).wait_recv()

    def rotated(u):
        return u * ctab[...] + pltpu.roll(u, HEAD // 2, 1) * stab[...]

    def block_decay(c, power):
        rows = [jnp.exp(jnp.full((R, HEAD), -power * B * rate[c * hc + h], F32)) for h in range(hc)]
        return jnp.concatenate(rows, axis=0)

    half = B // 2
    causal = (lax.broadcasted_iota(jnp.int32, (half, half), 0)
              >= lax.broadcasted_iota(jnp.int32, (half, half), 1))

    def kv_dots(c):
        for m in range(2):
            total = acc[m, c]
            for d in range(1, T):
                total = total + dot(xbuf[lax.rem(me + d, T)], wbuf[m, c, d])
            acc[m, c] = total

    def kv_finish(c):
        states = []
        for hh in range(hc):
            h = c * hc + hh
            cols = slice(hh * HEAD, (hh + 1) * HEAD)
            kr = rotated(acc[0, c, :, cols])
            tokk[h:h + 1, :] = kr[B:B + 1]
            krb = kr[:B].astype(BF)
            kbuf[h] = krb
            v = acc[1, c, :, cols]
            tokv[h:h + 1, :] = v[B:B + 1]
            vd = v[:B] * dec[h]
            vb = vd.astype(BF)
            vbuf[h] = (vd - jnp.mean(vd, axis=-1, keepdims=True)).astype(BF)
            first, second = (
                lax.dot_general(krb[lo:lo + half], vb[lo:lo + half], (((0,), (0,)), ((), ())), preferred_element_type=F32)
                for lo in (0, half))
            early[h] = first
            st = (first + second) * jnp.exp(jnp.full((HEAD, HEAD), -B * rate[h], F32))
            hi = st.astype(BF)
            shi[h] = hi
            slo[h] = (st - hi.astype(F32)).astype(BF)
            states.append(st)
        for i in range(G):
            for zz in range(Z):
                lo = (zz * G + i) * R
                send1[c, i, zz] = jnp.concatenate([s[lo:lo + R] for s in states], axis=0).astype(BF)
        recv1[c, j] = send1[c, j]

    def kv_send(c):
        for d in range(1, G):
            i = lax.rem(j + d, G)
            cp = pltpu.make_async_remote_copy(
                src_ref=send1.at[c, i], dst_ref=recv1.at[c, j], send_sem=s1s.at[0],
                recv_sem=s1r.at[c], device_id={"sp": z * G + i}, device_id_type=MESH)
            cp.start()

    def plane_wait(c):
        taken(recv1.at[c, pl.ds(0, G - 1)], s1r.at[c])

    def faded(c, p):
        rows = [jnp.exp(jnp.full((R, HEAD), -G * B * rate[c * hc + h], F32) * p) for h in range(hc)]
        return jnp.concatenate(rows, axis=0)[None]

    levels = (Z - 1).bit_length()

    def up_send(c, level):
        if level >= levels:
            return

        @pl.when(z % (2 << level) == (1 << level) - 1)
        def _():
            upb[c] = (tot[c] + exc[c] * faded(c, 1.0)).astype(BF)
            for k in range(1 << level, 0, -1):
                @pl.when(z + k < Z)
                def _():
                    pltpu.make_async_remote_copy(
                        src_ref=upb.at[c], dst_ref=uprecv.at[c, level], send_sem=us.at[0],
                        recv_sem=ur.at[c, level], device_id={"sp": (z + k) * G + j},
                        device_id_type=MESH).start()

    def plane(c):
        gb = block_decay(c, 1)[None]
        run = jnp.zeros((Z, hc * R, HEAD), F32)
        for i in range(G):
            pre[c, i] = run
            run = run * gb + recv1[c, i].astype(F32)
        tot[c] = run
        exc[c] = jnp.zeros((Z, hc * R, HEAD), F32)
        down[c] = run.astype(BF)
        for t in range(Z):
            @pl.when(t < z)
            def _():
                pltpu.make_async_remote_copy(
                    src_ref=down.at[c, t], dst_ref=downrecv.at[c, z], send_sem=ds.at[0],
                    recv_sem=dr.at[0], device_id={"sp": t * G + j}, device_id_type=MESH).start()
        up_send(c, 0)

        @pl.when(z == 0)
        def _():
            give_back(c)

    def climb(c, level):
        @pl.when((z // (1 << level)) % 2 == 1)
        def _():
            taken(uprecv.at[c, level], ur.at[c, level])
            p = (z % (1 << level)).astype(F32)
            exc[c] = exc[c] + uprecv[c, level].astype(F32) * faded(c, p)
        up_send(c, level + 1)

        @pl.when(z // (1 << level) == 1)
        def _():
            give_back(c)

    def give_back(c):
        run = exc[c]
        gb = block_decay(c, 1)[None]
        for i in range(G):
            send3[c, i] = (run + pre[c, i]).astype(BF)
            run = run * gb
        recv3[c, j] = send3[c, j]
        for d in range(1, G):
            i = lax.rem(j + d, G)
            cp = pltpu.make_async_remote_copy(
                src_ref=send3.at[c, i], dst_ref=recv3.at[c, j], send_sem=s3s.at[0],
                recv_sem=s3r.at[c], device_id={"sp": z * G + i}, device_id_type=MESH)
            cp.start()

    def final():
        for k in range(1, Z):
            @pl.when(Z - 1 - z == k)
            def _():
                taken(downrecv.at[:, pl.ds(0, k)], dr.at[0])
        for c in range(NC):
            gz = faded(c, 1.0)[0]
            run = tot[c, z] + exc[c, z] * gz
            for s in range(1, Z):
                run = jnp.where(s > z, run * gz + downrecv[c, s].astype(F32), run)
            for hh in range(hc):
                cache[c * hc + hh] = run[hh * R:(hh + 1) * R].astype(BF)

    def q_start(cs):
        row = (B + PAD) // 16 * 8
        for c in cs:
            for at in (slice(0, row), slice(row, B + PAD)):
                acc[0, c, at, :] = dot(xbuf[me, at, :], wbuf[2, c, 0])

    def q_project(cs, started):
        totals = []
        for c in cs:
            total = acc[0, c] if c in started else dot(xbuf[me], wbuf[2, c, 0])
            for d in range(1, T):
                total = total + dot(xbuf[lax.rem(me + d, T)], wbuf[2, c, d])
            totals.append(total)
        for c, total in zip(cs, totals):
            for hh in range(hc):
                h = c * hc + hh
                qr = rotated(total[:, hh * HEAD:(hh + 1) * HEAD])
                tokq[h:h + 1, :] = qr[B:B + 1]
                qbuf[h] = qr[:B].astype(BF)

    def attend(c):
        for hh in range(hc):
            h = c * hc + hh
            for lo in (0, half):
                at = slice(lo, lo + half)
                sc = lax.dot_general(
                    qbuf[h, at, :], kbuf[h, at, :], (((1,), (1,)), ((), ())), preferred_element_type=F32)
                sc = jnp.where(causal, sc, 0.0).astype(BF)
                intra[h, at, :] = dot(sc, vbuf[h, at, :])

    def tail_wait(c):
        taken(recv3.at[c, pl.ds(0, G - 1)], s3r.at[c])

    def tail(c):
        pieces = [[recv3[c, i, zz].astype(F32) for i in range(G)] for zz in range(Z)]
        for hh in range(hc):
            h = c * hc + hh
            inc = jnp.concatenate(
                [pieces[zz][i][hh * R:(hh + 1) * R] for zz in range(Z) for i in range(G)], axis=0)
            for lo in (0, half):
                at = slice(lo, lo + half)
                held = inc if lo == 0 else inc + early[h]
                held = (held - jnp.mean(held, axis=-1, keepdims=True)).astype(BF)
                delta = intra[h, at, :] + dot(qbuf[h, at, :], held)
                spread = jnp.mean(delta * delta, axis=-1, keepdims=True)
                res = delta * lax.rsqrt(spread + floor[h, at, :]) * gain[:, h * HEAD:(h + 1) * HEAD]
                mixed[at, h * HEAD:(h + 1) * HEAD] = res.astype(BF)

    def read_send():
        tq = jnp.concatenate([tokq[...], tokq[...]], axis=0).astype(BF)
        later = (M - 1 - rank).astype(F32)
        for h in range(H):
            got = dot(tq, shi[h]) + dot(tq, slo[h])
            fade = jnp.exp(jnp.full((1, HEAD), -B * rate[h], F32) * later)
            rd1[j, h:h + 1, :] = got[h:h + 1] * fade
        for d in range(1, G):
            pltpu.make_async_remote_copy(
                src_ref=rd1.at[j], dst_ref=rd1.at[j], send_sem=rds.at[0], recv_sem=rdr.at[0],
                device_id={"sp": z * G + lax.rem(j + d, G)}, device_id_type=MESH).start()
        for t in range(Z - 1):
            @pl.when(t < z)
            def _():
                for i in range(G):
                    pltpu.make_async_remote_copy(
                        src_ref=rd1.at[j], dst_ref=rd3.at[rank], send_sem=rds.at[1], recv_sem=rdr.at[1],
                        device_id={"sp": t * G + i}, device_id_type=MESH).start()

    def read_relay():
        taken(rd1.at[pl.ds(0, G - 1)], rdr.at[0])
        rd2[z] = jnp.sum(rd1[...], axis=0)
        for t in range(1, Z):
            @pl.when(t > z)
            def _():
                pltpu.make_async_remote_copy(
                    src_ref=rd2.at[z], dst_ref=rd2.at[z], send_sem=rds.at[2], recv_sem=rdr.at[2],
                    device_id={"sp": t * G + j}, device_id_type=MESH).start()

    def read_finish():
        for k in range(1, Z):
            @pl.when(Z - 1 - z == k)
            def _():
                taken(rd3.at[pl.ds(0, k * G)], rdr.at[1])

            @pl.when(z == k)
            def _():
                taken(rd2.at[pl.ds(0, k)], rdr.at[2])
        total = rd2[z]
        for t in range(Z):
            if t < Z - 1:
                total = total + jnp.where(t < z, rd2[t], 0.0)
            if t > 0:
                total = total + jnp.where(t > z, jnp.sum(rd3[t * G:(t + 1) * G], axis=0), 0.0)
        scale = HEAD ** -0.5
        tq = tokq[...].astype(BF).astype(F32)
        tk = tokk[...].astype(BF).astype(F32)
        score = jnp.sum(tq * tk, axis=-1, keepdims=True) * scale
        base_part = score * tokv[...].astype(BF).astype(F32)
        for h in range(H):
            g = jnp.exp(jnp.full((1, HEAD), -rate[h], F32)) * scale
            o = g * total[h:h + 1] + base_part[h:h + 1]
            read_out[:, h * HEAD:(h + 1) * HEAD] = head_norm(o, gain[:, h * HEAD:(h + 1) * HEAD]).astype(BF)

    def before_q():
        with jax.named_scope("w_up"):
            @pl.when(z < Z - 1)
            def _():
                pl.semaphore_wait(up_sem, Z - 1 - z)
        lg.wait()
        with jax.named_scope("w_wq"):
            taken(wbuf.at[2], w_sem.at[NC + 1])

    def planes(cs):
        for c in cs:
            with jax.named_scope(f"w_plane{c}"):
                plane_wait(c)
            with jax.named_scope(f"plane{c}"):
                plane(c)

    def attends(cs):
        for c in cs:
            with jax.named_scope(f"att{c}"):
                attend(c)

    def climbs(cs, level):
        for c in cs:
            with jax.named_scope(f"climb{c}_{level}"):
                climb(c, level)

    for c in range(NC):
        if c == NC - 1:
            before_q()
        with jax.named_scope(f"kv{c}"):
            kv_dots(c)
            if c > 0:
                kv_finish(c - 1)
                kv_send(c - 1)
    started = list(range(min(1, NC - 1)))
    with jax.named_scope("kvlast"):
        q_start(started)
        kv_finish(NC - 1)
        kv_send(NC - 1)
    groups = [range(c, min(c + 2, NC)) for c in range(0, NC, 2)]
    ready = 0
    for n, cs in enumerate(groups):
        with jax.named_scope(f"q{n}"):
            q_project(cs, started)
        if n < len(groups) - 1:
            for c in cs:
                attends([c])
                planes([ready])
                ready += 1
    planes(range(ready, NC))
    with jax.named_scope("rsend"):
        read_send()
    rest = list(groups[-1])
    step = 0
    if levels > 0:
        climbs(range(min(1, NC - 1)), 0)
        step = 1
    for c in rest:
        attends([c])
        if levels > 0:
            more = NC if c == rest[-1] else min(step + 1, NC)
            climbs(range(step, min(more, NC - 1)), 0)
            step = more
    if levels > 1:
        climbs([0], 1)
    if levels > 0:
        climbs([NC - 1], 0)
    for level in range(1, levels):
        climbs(range(1 if level == 1 else 0, NC), level)
    with jax.named_scope("w_relay"):
        read_relay()
    middle = Z // 2

    @pl.when(z >= middle)
    def _():
        with jax.named_scope("finala"):
            final()
    for n, cs in enumerate(groups):
        with jax.named_scope(f"w_tail{cs[0]}"):
            for c in cs:
                tail_wait(c)
        with jax.named_scope(f"tail{cs[0]}"):
            for c in cs:
                tail(c)
        if n == 0:
            @pl.when(z >= middle)
            def _():
                with jax.named_scope("w_rfina"):
                    read_finish()

    @pl.when(z < middle)
    def _():
        with jax.named_scope("final"):
            final()
        with jax.named_scope("w_rfin"):
            read_finish()
    with jax.named_scope("w_sends"):
        for cp in sends:
            cp.wait_send()
        taken(send1.at[:, pl.ds(0, G - 1)], s1s.at[0])
        taken(send3.at[:, pl.ds(0, G - 1)], s3s.at[0])
        taken(rd1.at[pl.ds(0, G - 1)], rds.at[0])
        for k in range(1, Z):
            @pl.when(z == k)
            def _():
                taken(down.at[:, pl.ds(0, k)], ds.at[0])
                taken(rd3.at[pl.ds(0, k * G)], rds.at[1])

            @pl.when(Z - 1 - z == k)
            def _():
                taken(rd2.at[pl.ds(0, k)], rds.at[2])
        for k in range(Z - 1):
            level = ((k + 1) & -(k + 1)).bit_length() - 1
            count = min(1 << level, Z - 1 - k)

            @pl.when(z == k)
            def _():
                taken(uprecv.at[:, pl.ds(0, 1)] if count == 1 else recv1.at[:, pl.ds(0, count)], us.at[0])


def flush(*refs):
    n = (len(refs) - 1) // 2
    sems = refs[-1]
    copies = []
    for i in range(n):
        rows = refs[i].shape[0]
        pieces = 4 if i == 0 else 1
        for k in range(pieces):
            at = pl.ds(k * (rows // pieces), rows // pieces)
            copies.append(pltpu.make_async_copy(refs[i].at[at], refs[n + i].at[at], sems.at[len(copies)]))
    for cp in copies:
        cp.start()
    for cp in copies:
        cp.wait()


def per_device(prompt, new_token, w_query, w_key, w_value, decay_rate, norm_gain):
    _, B, F = prompt.shape
    H = w_query.shape[1] // HEAD
    M = lax.axis_size("sp")
    T = lax.axis_size("tp")
    G = split(M)
    Z = M // G
    R = HEAD // M
    hc = 2 if H % 2 == 0 else 1
    NC = H // hc
    W = hc * HEAD
    inverse = rope_base ** (-np.arange(0, HEAD, 2, dtype=np.float64) / HEAD)
    sign = np.concatenate([-np.ones(HEAD // 2), np.ones(HEAD // 2)])

    def pair(positions):
        angles = np.concatenate([positions[:, None] * inverse[None]] * 2, axis=1)
        return np.cos(angles), np.sin(angles) * sign[None]

    tab = np.stack(pair(np.arange(B, dtype=np.float64))).astype(np.float32)
    base = np.stack(pair(np.arange(M + 1, dtype=np.float64) * B), axis=1).astype(np.float32)
    tab = np.concatenate([tab.reshape(2 * B, HEAD), np.repeat(base.reshape(2 * (M + 1), HEAD), 8, axis=0)])
    levels = (Z - 1).bit_length()
    any_ = pl.BlockSpec(memory_space=pltpu.HBM)
    vm = pl.BlockSpec(memory_space=pltpu.VMEM)
    V = pltpu.VMEM
    DMA = pltpu.SemaphoreType.DMA
    cfg = (M, G, Z, T, B, F, H, hc, R)
    shapes = ((B, H * HEAD), (H, R, HEAD), (1, H * HEAD))
    held = pl.pallas_call(
        functools.partial(kernel, cfg),
        out_shape=tuple(V(shape, BF) for shape in shapes),
        in_specs=[any_] * 8,
        out_specs=(vm, vm, vm),
        scratch_shapes=[
            pltpu.SMEM((H,), F32),
            V((T, B + PAD, F), BF),
            V((3, NC, T, F, W), BF),
            V((2, NC, B + PAD, W), F32),
            V(tab.shape, F32),
            V((1, H * HEAD), F32),
            V((B + PAD, HEAD), F32),
            V((B + PAD, HEAD), F32),
            V((H, B, HEAD), F32),
            V((H, B, HEAD), F32),
            V((H, B, HEAD), BF),
            V((H, B, HEAD), BF),
            V((H, B, HEAD), BF),
            V((H, HEAD, HEAD), F32),
            V((H, HEAD, HEAD), BF),
            V((H, HEAD, HEAD), BF),
            V((H, B, HEAD), F32),
            V((NC, G, Z, hc * R, HEAD), BF),
            V((NC, G, Z, hc * R, HEAD), BF),
            V((NC, G, Z, hc * R, HEAD), F32),
            V((NC, Z, hc * R, HEAD), F32),
            V((NC, Z, hc * R, HEAD), F32),
            V((NC, Z, hc * R, HEAD), BF),
            V((NC, max(levels, 1), Z, hc * R, HEAD), BF),
            V((NC, Z, hc * R, HEAD), BF),
            V((NC, Z, hc * R, HEAD), BF),
            V((NC, G, Z, hc * R, HEAD), BF),
            V((NC, G, Z, hc * R, HEAD), BF),
            V((H, HEAD), F32),
            V((H, HEAD), F32),
            V((H, HEAD), F32),
            V((G, H, HEAD), F32),
            V((Z, H, HEAD), F32),
            V((M, H, HEAD), F32),
            V((1, F), BF),
            DMA((NC + 2,)),
            DMA((5,)),
            DMA((max(T - 1, 1),)),
            DMA((max(T - 1, 1),)),
            DMA((1,)),
            DMA((NC,)),
            DMA((1,)),
            DMA((NC, max(levels, 1))),
            DMA((1,)),
            DMA((1,)),
            DMA((1,)),
            DMA((NC,)),
            DMA((3,)),
            DMA((3,)),
            pltpu.SemaphoreType.REGULAR,
        ],
        compiler_params=pltpu.CompilerParams(
            collective_id=0, has_side_effects=True, vmem_limit_bytes=60 * 1024 * 1024),
    )(prompt.reshape(B, F), new_token, w_query, w_key, w_value, decay_rate,
      norm_gain.reshape(1, H * HEAD), jnp.asarray(tab, F32))
    mixed, cache, new_read = pl.pallas_call(
        flush,
        out_shape=tuple(jax.ShapeDtypeStruct(shape, BF) for shape in shapes),
        in_specs=[vm] * len(shapes),
        out_specs=(any_,) * len(shapes),
        scratch_shapes=[DMA((len(shapes) + 3,))],
    )(*(pltpu.with_memory_space_constraint(a, V) for a in held))
    return (mixed[None], cache[None], new_read)


def solution(mesh):
    in_specs = (
        P(None, "sp", "tp"),
        P(None, "tp"),
        P(None, "tp"),
        P(None, "tp"),
        P(None, "tp"),
        P("tp"),
        P("tp"),
    )
    out_specs = (P(None, "sp", "tp"), P(None, "tp", "sp", None), P(None, "tp"))
    return jax.shard_map(
        per_device, mesh=mesh, in_specs=in_specs, out_specs=out_specs, check_vma=False
    )
```
